32 devices in a mesh: ep: 8 (over z, y), tp: 4 (over x, core).
Axes of the slice: x: 2, y: 2, z: 4, core: 2. Of those that a mesh axis runs over, the one named last changes fastest.
Arguments:
- tokens: bfloat16 [1024, 2048], P('ep'), may hold values from -6 to 6
- out_grad: bfloat16 [1024, 2048], P('ep'), may hold values from -50 to 50
- expert_ids: int32 [1024, 2], P('ep'), may hold values from 0 to 7, all different within a row; in each aligned block of 128 rows (0 to 127, 128 to 255, ...) at most 40 rows name the same one
- route_weights: float32 [1024, 2], P('ep'), may hold values from 0.2 to 2
- gate_proj: bfloat16 [8, 2048, 2048], P('ep', 'tp'), may hold values from -0.125 to 0.125
- up_proj: bfloat16 [8, 2048, 2048], P('ep', 'tp'), may hold values from -0.125 to 0.125
- down_proj: bfloat16 [8, 2048, 2048], P('ep', 'tp'), may hold values from -0.125 to 0.125
- shared_act: bfloat16 [1024, 1024], P('ep'), may hold values from -0.29882812 to 0.29882812
Outputs:
- token_grad: bfloat16 [1024, 2048], P('ep', 'tp')
- route_grad: float32 [1024, 2], P('ep')
- gate_grad: bfloat16 [8, 2048, 2048], P('ep', 'tp')
- up_grad: bfloat16 [8, 2048, 2048], P('ep', 'tp')
- down_grad: bfloat16 [8, 2048, 2048], P('ep', 'tp')
- row_norms: float32 [8, 3, 2048], P('ep', None, 'tp')
- shared_grad: float32 [1024, 2048], P('tp', 'ep')
- shared_norms: float32 [1024], P('tp')
The draws below stay inside these ranges and needn't reach their ends.
Inputs may be any that keep to these rules, and one draw needn't show every extreme that they name: `expert_ids`: each row names 2 different experts. In the rows of one device no expert is named more than 40 times, and in some device some expert is named exactly 40 times.
All inputs are finite; a program needn't handle non-finite values.
Results may differ from the reference program's by a relative error of at most 0.008.
Values may be sent and summed in bfloat16 or wider, within the bound.
A program may use at most 64 MiB of HBM per device.

```python
import math
import jax
import jax.numpy as jnp
import numpy as np
from jax import lax

D = 2048
F = 2048
SH = 1024
TOPK = 2
TOK_DEV = 128
EXPERTS = 8
TOKENS = 1024
CAP = 40
N_EP = 8
N_TP = 4


def draw_out_grad(key, part):
    key_cols = jax.random.fold_in(key, 11)
    key_rows = jax.random.fold_in(key, 12)
    key_base = jax.random.fold_in(key, 13)
    position = jnp.arange(D, dtype=jnp.float32) / max(D - 1, 1)
    col_scale = jnp.exp(position * jnp.log(3.0)) * jnp.exp(jax.random.uniform(key_cols, (D,), jnp.float32, -1.2, 1.2))
    row_scale = jnp.exp(jax.random.uniform(key_rows, (TOKENS, 1), jnp.float32, -1.2, 1.2))
    base = jnp.clip(jax.random.normal(key_base, (TOKENS, D), jnp.float32), -6.0, 6.0)
    return (0.25 * base * row_scale * col_scale[None, :]).astype(jnp.bfloat16)


def steps_of(own_key, extent, shards, smallest, top_value):
    loudness, own = 1.0, jax.random.fold_in(own_key, 6)
    for axis_at, shards_of in shards:
        steps = jnp.exp(jax.random.uniform(jax.random.fold_in(own, axis_at), (shards_of,), jnp.float32, smallest / len(shards), top_value / len(shards)))
        loudness = loudness * jnp.repeat(steps, extent[axis_at] // shards_of).reshape([-1 if axis == axis_at else 1 for axis in range(len(extent))])
    return loudness


def routed_block(key, own, number, rows, amount, top, most, lean):
    ranking = jax.random.permutation(key, amount)
    crowded, usual = load_shares(amount, rows * top, most, lean, True), load_shares(amount, rows * top, most, lean, False)
    places = jnp.arange(amount)

    def named(tallies, offset_by):
        used = int((tallies > 0).sum())
        fixed = max(1, used // 4)
        moved = fixed + (places - fixed + offset_by * (used - fixed)) % max(1, amount - fixed)
        return jnp.zeros((amount,), jnp.int32).at[ranking[jnp.where(places < fixed, places, moved)]].set(jnp.asarray(tallies, jnp.int32))

    tallies = jnp.where(number % 4 == 0, named(crowded, number // 4), named(usual, number - number // 4 - 1))
    mixed = jax.random.permutation(jax.random.fold_in(own, 3), amount)
    donor, taker = mixed[0:amount // 2 * 2:2], mixed[1:amount // 2 * 2:2]
    slack = jnp.minimum(tallies[donor] - 1, most - tallies[taker]) // 2
    slack = jnp.where((donor == ranking[0]) | (taker == ranking[0]) | (tallies[taker] == 0), 0, jnp.maximum(slack, 0))
    moved = jax.random.randint(jax.random.fold_in(own, 4), (amount // 2,), 0, 1 << 20) % (slack + 1)
    tallies = tallies.at[donor].add(-moved).at[taker].add(moved)
    members = jnp.searchsorted(jnp.cumsum(tallies), jnp.arange(rows * top), side="right").astype(jnp.int32)
    listing = members.reshape(top, rows).T
    listing = listing[jax.random.permutation(jax.random.fold_in(own, 1), rows)]
    offset_by = jax.random.randint(jax.random.fold_in(own, 2), (rows, 1), 0, top)
    return jnp.take_along_axis(listing, (jnp.arange(top)[None, :] + offset_by) % top, axis=1)


def load_shares(count, total, bound, lean, full):
    portions = [(1 << 20) // math.isqrt(rank ** lean) + 1 for rank in range(1, count + 1)]
    largest = bound if full else min(bound, max(-(-total // count), total * portions[0] // sum(portions)))
    least = 1 if total - largest >= count - 1 else 0
    counts, spare = [largest] + [least] * (count - 1), total - largest - least * (count - 1)
    while spare > 0:
        candidates = [i for i in range(1, count) if counts[i] < largest] or [i for i in range(1, count) if counts[i] < bound]
        pool, budget = sum([portions[i] for i in candidates]), spare
        for i in candidates:
            more = min(bound - counts[i], max(1, budget * portions[i] // pool), spare)
            counts[i] = counts[i] + more
            spare = spare - more
    return np.array(counts)


def scatter_about(rng, dims, scale, bound, split=(), kind=jnp.bfloat16):
    entries = jax.random.normal(rng, dims, jnp.float32) * scale
    if len(split) > 0:
        entries = steps_of(rng, dims, split, -0.22, 0.18) * entries
    return jnp.clip(entries, min=-bound, max=bound).astype(kind)


def setup_inputs(seed: int = 0) -> dict:
    keys = jax.random.split(jax.random.key(seed), 9)
    tokens = scatter_about(keys[0], (TOKENS, D), 1.0, 6.0, ((0, 8),))
    out_grad = draw_out_grad(jax.random.fold_in(keys[8], 71), 0)
    expert_ids_keys = jax.random.split(jax.random.fold_in(keys[2], 1), TOKENS // TOK_DEV)
    expert_ids_turns = jax.random.permutation(jax.random.fold_in(keys[2], 3), TOKENS // TOK_DEV)
    expert_ids = jax.vmap(lambda own, number: routed_block(jax.random.fold_in(keys[2], 2), own, number, TOK_DEV, EXPERTS, TOPK, CAP, 2))(expert_ids_keys, expert_ids_turns).reshape((TOKENS, TOPK))
    route_weights = jnp.clip(jnp.exp(math.log(2.0) - 2.3025851 * jax.random.uniform(keys[3], (TOKENS, TOPK), jnp.float32) ** steps_of(keys[3], (TOKENS, TOPK), ((0, 8),), -0.2, 0.2)), 0.2, 2.0)
    gate_proj = scatter_about(keys[4], (EXPERTS, F, D), D ** -0.5, 0.125, ((0, 8), (1, 4)))
    up_proj = scatter_about(keys[5], (EXPERTS, F, D), D ** -0.5, 0.125, ((0, 8), (1, 4)))
    down_proj = scatter_about(keys[6], (EXPERTS, F, D), D ** -0.5, 0.125, ((0, 8), (1, 4)))
    shared_act = scatter_about(keys[7], (TOKENS, SH), 0.05, 0.29882812, ((0, 8),))
    return {"tokens": tokens, "out_grad": out_grad, "expert_ids": expert_ids, "route_weights": route_weights, "gate_proj": gate_proj, "up_proj": up_proj, "down_proj": down_proj, "shared_act": shared_act}


def expert_pass(tokens, scaled, index_row, gate_w, up_w, down_w):
    valid = index_row >= 0
    safe = jnp.where(valid, index_row, 0)
    rows_in = jnp.where(valid[:, None], tokens[safe // TOPK], jnp.zeros((), tokens.dtype))
    rows_cot = jnp.where(valid[:, None], scaled[safe], jnp.zeros((), scaled.dtype))
    gate_pre = jnp.dot(rows_in, gate_w.T, preferred_element_type=jnp.float32)
    up_pre = jnp.dot(rows_in, up_w.T, preferred_element_type=jnp.float32)
    sigmoid_a = jax.nn.sigmoid(gate_pre)
    silu_a = gate_pre * sigmoid_a
    hidden = (silu_a * up_pre).astype(jnp.bfloat16)
    hidden_grad = jnp.dot(rows_cot, down_w.T, preferred_element_type=jnp.float32)
    up_delta = (hidden_grad * silu_a).astype(jnp.bfloat16)
    gate_delta = (hidden_grad * up_pre * sigmoid_a * (1.0 + gate_pre * (1.0 - sigmoid_a))).astype(jnp.bfloat16)
    gate_full = jnp.dot(gate_delta.T, rows_in, preferred_element_type=jnp.float32)
    up_full = jnp.dot(up_delta.T, rows_in, preferred_element_type=jnp.float32)
    down_full = jnp.dot(hidden.T, rows_cot, preferred_element_type=jnp.float32)
    norm_rows = jnp.stack([jnp.sum(gate_full * gate_full, 1), jnp.sum(up_full * up_full, 1),
                           jnp.sum(down_full * down_full, 1)])
    row_count = index_row.shape[0]
    block = F // N_TP
    partial_value = jnp.einsum('rbf,bfd->rbd', gate_delta.astype(jnp.float32).reshape(row_count, N_TP, block),
                         gate_w.astype(jnp.float32).reshape(N_TP, block, D))
    partial_value = partial_value + jnp.einsum('rbf,bfd->rbd', up_delta.astype(jnp.float32).reshape(row_count, N_TP, block),
                                   up_w.astype(jnp.float32).reshape(N_TP, block, D))
    partial_value = lax.optimization_barrier(partial_value.astype(jnp.bfloat16)).astype(jnp.float32)
    slot_grad = jnp.sum(partial_value, 1)
    inner_part = (hidden.astype(jnp.float32) * hidden_grad).reshape(row_count, N_TP, block).sum(-1)
    inner_part = lax.optimization_barrier(inner_part.astype(jnp.bfloat16)).astype(jnp.float32)
    inner = jnp.sum(inner_part, 1)
    return (gate_full.astype(jnp.bfloat16), up_full.astype(jnp.bfloat16), down_full.astype(jnp.bfloat16),
            norm_rows, slot_grad, inner)


def reference(tokens, out_grad, expert_ids, route_weights, gate_proj, up_proj, down_proj, shared_act):
    per_dev = TOK_DEV * TOPK
    chosen = expert_ids.reshape(N_EP, per_dev).astype(jnp.int32)
    onehot = (chosen[..., None] == jnp.arange(EXPERTS, dtype=jnp.int32)[None, None, :]).astype(jnp.int32)
    before = jnp.cumsum(onehot, axis=1) - onehot
    rank_in = jnp.sum(before * onehot, -1).astype(jnp.int32)
    row_at = (jnp.arange(N_EP, dtype=jnp.int32)[:, None] * CAP + rank_in).astype(jnp.int32)
    global_id = jnp.arange(N_EP * per_dev, dtype=jnp.int32).reshape(N_EP, per_dev)
    table = jnp.full((EXPERTS, N_EP * CAP), -1, jnp.int32).at[chosen, row_at].set(global_id)
    scaled = (route_weights[:, :, None] * out_grad[:, None, :].astype(jnp.float32)).astype(jnp.bfloat16)
    scaled = scaled.reshape(TOKENS * TOPK, D)

    def one_expert(packed):
        index_row, gate_w, up_w, down_w = packed
        return expert_pass(tokens, scaled, index_row, gate_w, up_w, down_w)

    gate_grad, up_grad, down_grad, row_norms, slot_grads, inners = lax.map(
        one_expert, (table, gate_proj, up_proj, down_proj))
    target = jnp.where(table >= 0, table, TOKENS * TOPK).reshape(-1)
    assign_grad = jnp.zeros((TOKENS * TOPK + 1, D), jnp.float32).at[target].add(slot_grads.reshape(-1, D))
    assign_inner = jnp.zeros((TOKENS * TOPK + 1,), jnp.float32).at[target].add(inners.reshape(-1))
    token_grad = assign_grad[:TOKENS * TOPK].reshape(TOKENS, TOPK, D).sum(1).astype(jnp.bfloat16)
    route_grad = assign_inner[:TOKENS * TOPK].reshape(TOKENS, TOPK) / route_weights
    shared_grad = jnp.dot(shared_act.T, out_grad, preferred_element_type=jnp.float32)
    shared_norms = jnp.sum(shared_grad * shared_grad, 1)
    return (token_grad, route_grad, gate_grad, up_grad, down_grad, row_norms, shared_grad, shared_norms)
```

```python
import functools

import jax
import jax.numpy as jnp
from jax import lax
from jax.experimental import pallas as pl
from jax.experimental.pallas import tpu as pltpu
from jax.sharding import PartitionSpec as P


def plain(tokens, out_grad, expert_ids, route_weights, gate_proj, up_proj, down_proj, shared_act):
    ep_count = lax.axis_size("ep")
    tp_count = lax.axis_size("tp")
    tok_count, model_width = tokens.shape
    top_count = expert_ids.shape[1]
    exp_local = gate_proj.shape[0]
    experts = exp_local * ep_count
    capacity = 5 * tok_count * top_count // (4 * experts)
    slot_count = experts * capacity
    assign = tok_count * top_count
    columns = model_width // tp_count
    offset = lax.axis_index("tp") * columns
    flat_expert = expert_ids.reshape(assign)
    onehot = (flat_expert[:, None] == jnp.arange(experts, dtype=jnp.int32)[None, :]).astype(
        jnp.float32
    )
    earlier = (jnp.arange(assign)[:, None] > jnp.arange(assign)[None, :]).astype(jnp.float32)
    counted = jnp.dot(earlier, onehot, precision=lax.Precision.HIGHEST)
    rank_in = jnp.sum(counted * onehot, 1).astype(jnp.int32)
    slot_id = flat_expert * capacity + rank_in
    picked = (jnp.arange(slot_count, dtype=jnp.int32)[:, None] == slot_id[None, :]).astype(
        jnp.float32
    )
    source_id = jnp.dot(
        picked, jnp.arange(assign, dtype=jnp.float32), precision=lax.Precision.HIGHEST
    ).astype(jnp.int32)
    filled = jnp.sum(picked, 1) > 0.5
    scaled = (
        (route_weights[:, :, None] * out_grad[:, None, :])
        .astype(jnp.bfloat16)
        .reshape(assign, model_width)
    )

    def slot_rows(source_rows, row_index):
        taken = jnp.take(source_rows, row_index, axis=0)
        return jnp.where(filled[:, None], taken, jnp.zeros((), source_rows.dtype))

    token_part = lax.dynamic_slice_in_dim(tokens, offset, columns, 1)
    scaled_part = lax.dynamic_slice_in_dim(scaled, offset, columns, 1)
    send_in = slot_rows(token_part, source_id // top_count).reshape(
        ep_count, exp_local, capacity, columns
    )
    send_cot = slot_rows(scaled_part, source_id).reshape(ep_count, exp_local, capacity, columns)
    part_in, part_cot = (
        lax.all_to_all(send_in, "ep", split_axis=0, concat_axis=2, tiled=True),
        lax.all_to_all(send_cot, "ep", split_axis=0, concat_axis=2, tiled=True),
    )
    joined_in, joined_cot = (
        lax.all_gather(part_in, "tp", axis=3, tiled=True),
        lax.all_gather(part_cot, "tp", axis=3, tiled=True),
    )
    rows_in = joined_in[0]
    rows_cot = joined_cot[0]
    gate_pre = jnp.einsum("erd,efd->erf", rows_in, gate_proj, preferred_element_type=jnp.float32)
    up_pre = jnp.einsum("erd,efd->erf", rows_in, up_proj, preferred_element_type=jnp.float32)
    sigmoid_a = jax.nn.sigmoid(gate_pre)
    silu_a = gate_pre * sigmoid_a
    hidden = (silu_a * up_pre).astype(jnp.bfloat16)
    hidden_grad = jnp.einsum(
        "erd,efd->erf", rows_cot, down_proj, preferred_element_type=jnp.float32
    )
    up_delta = (hidden_grad * silu_a).astype(jnp.bfloat16)
    gate_delta = (hidden_grad * up_pre * sigmoid_a * (1.0 + gate_pre * (1.0 - sigmoid_a))).astype(
        jnp.bfloat16
    )
    gate_full = jnp.einsum("erf,erd->efd", gate_delta, rows_in, preferred_element_type=jnp.float32)
    up_full = jnp.einsum("erf,erd->efd", up_delta, rows_in, preferred_element_type=jnp.float32)
    down_full = jnp.einsum("erf,erd->efd", hidden, rows_cot, preferred_element_type=jnp.float32)
    row_norms = jnp.stack(
        [
            jnp.sum(gate_full * gate_full, 2),
            jnp.sum(up_full * up_full, 2),
            jnp.sum(down_full * down_full, 2),
        ],
        axis=1,
    )
    row_total = rows_in.shape[1]
    partial_value = jnp.einsum(
        "erf,efd->erd", gate_delta, gate_proj, preferred_element_type=jnp.float32
    )
    partial_value = partial_value + jnp.einsum(
        "erf,efd->erd", up_delta, up_proj, preferred_element_type=jnp.float32
    )
    partials = partial_value.astype(jnp.bfloat16).reshape(exp_local, row_total, tp_count, columns)
    inner_part = jnp.sum(hidden.astype(jnp.float32) * hidden_grad, 2).astype(jnp.bfloat16)
    inner_parts = jnp.broadcast_to(inner_part[:, :, None], (exp_local, row_total, tp_count))
    received, received_inner = (
        lax.all_to_all(partials, "tp", split_axis=2, concat_axis=2, tiled=True),
        lax.all_to_all(inner_parts, "tp", split_axis=2, concat_axis=2, tiled=True),
    )
    slot_grad = jnp.sum(received.astype(jnp.float32), 2)
    inner = jnp.sum(received_inner.astype(jnp.float32), 2)
    returned, returned_inner = (
        lax.all_to_all(
            slot_grad.reshape(exp_local, ep_count, capacity, columns),
            "ep",
            split_axis=1,
            concat_axis=0,
            tiled=True,
        ),
        lax.all_to_all(
            inner.reshape(exp_local, ep_count, capacity),
            "ep",
            split_axis=1,
            concat_axis=0,
            tiled=True,
        ),
    )
    slot_back = returned.reshape(slot_count, columns)
    inner_back = returned_inner.reshape(slot_count)
    token_grad = jnp.take(slot_back, slot_id, axis=0).reshape(tok_count, top_count, columns).sum(1)
    route_grad = jnp.take(inner_back, slot_id).reshape(tok_count, top_count) / route_weights
    shared_rows = shared_act.shape[1] // tp_count
    shared_part = lax.dynamic_slice_in_dim(
        shared_act, lax.axis_index("tp") * shared_rows, shared_rows, 1
    )
    shared_term = lax.dot_general(
        shared_part, out_grad, (((0,), (0,)), ((), ())), preferred_element_type=jnp.float32
    )
    shared_grad = lax.psum_scatter(shared_term, "ep", scatter_dimension=1, tiled=True)
    shared_norms = lax.psum(jnp.sum(shared_grad * shared_grad, 1), "ep")
    return (
        token_grad.astype(jnp.bfloat16),
        route_grad,
        gate_full.astype(jnp.bfloat16),
        up_full.astype(jnp.bfloat16),
        down_full.astype(jnp.bfloat16),
        row_norms,
        shared_grad,
        shared_norms,
    )


MESH = pl.DeviceIdType.MESH
F32 = jnp.float32
BF16 = jnp.bfloat16
NT = (((1,), (1,)), ((), ()))


def column_to_row(col, width=128):
    return jnp.broadcast_to(col, (col.shape[0], width)).T[0:1]


def kernel(
    n, t, cap, slot,
    ids_ref, rw_ref, tok_hbm, og_hbm, act_hbm, wg_hbm, wu_hbm, wd_hbm,
    token_out, route_out, gate_out, up_out, down_out, norms_out, shared_out, snorm_out,
    send, rows, wg, wu, wd, picks, delta, turned, squares,
    pair_send, pair_recv, acc_far, acc_own, far_send, far_recv, back_send, back_recv,
    inner_tp, inner_tot, inner_ep, act_send, act_all, og_send, og_all, snorm_all,
    tok_part, og_part, og_mine, act_part, l_sem,
    w_sem, d_s, d_r, m_s, m_r, c_s, c_r, a_s, a_r, o_s, o_r, q_s, q_r,
    p_s, p_r, f_s, f_r, b_s, b_r, i_s, i_r, j_s, j_r, n_s, n_r,
):
    me = lax.axis_index("ep")
    p = lax.axis_index("tp")
    buddy = p + 1 - 2 * lax.rem(p, 2)
    half = t // 2
    mirror = lax.rem(p + half, t)
    mirror_buddy = lax.rem(buddy + half, t)
    toks, width = tok_hbm.shape
    cols = width // t
    hid = wg.shape[0]
    total = n * slot

    def span(q, size):
        return pl.ds(pl.multiple_of(q * size, 128), size)

    def ahead(i):
        out, bit = 0, 1
        while bit < n:
            digit = lax.rem(me // bit, 2)
            out = out + bit * (1 - digit if i // bit % 2 else digit)
            bit *= 2
        return out

    behind = ahead

    def tp_ahead(i):
        return lax.rem(p + i, t)

    def tp_behind(i):
        return lax.rem(p - i + t, t)

    def copy(src, dst, s_sem, r_sem, where):
        return pltpu.make_async_remote_copy(
            src_ref=src, dst_ref=dst, send_sem=s_sem, recv_sem=r_sem,
            device_id=where, device_id_type=MESH,
        )

    weights = [
        pltpu.make_async_copy(wg_hbm.at[0], wg, w_sem.at[0]),
        pltpu.make_async_copy(wu_hbm.at[0], wu, w_sem.at[1]),
        pltpu.make_async_copy(wd_hbm.at[0], wd, w_sem.at[2]),
    ]
    part = toks // t
    sh = act_hbm.shape[1] // t
    cut = width // n
    loads = [
        pltpu.make_async_copy(tok_hbm.at[:, span(p, cols)], tok_part, l_sem.at[0]),
        pltpu.make_async_copy(og_hbm.at[:, span(p, cols)], og_part, l_sem.at[1]),
        pltpu.make_async_copy(
            og_hbm.at[pl.ds(pl.multiple_of(p * part, 16), part), :], og_mine, l_sem.at[2]
        ),
        pltpu.make_async_copy(act_hbm.at[:, span(p, sh)], act_part, l_sem.at[3]),
    ]
    for load in loads:
        load.start()
    if slot != cap:
        rows[:, :, cap:, :] = jnp.zeros((2, n, slot - cap, width), BF16)
    barrier = pltpu.get_barrier_semaphore()
    for i in range(1, n):
        pl.semaphore_signal(barrier, inc=1, device_id={"ep": ahead(i)}, device_id_type=MESH)
    for i in range(1, t):
        pl.semaphore_signal(barrier, inc=1, device_id={"tp": tp_ahead(i)}, device_id_type=MESH)
    for w in weights:
        w.start()

    expert = lax.broadcasted_iota(jnp.int32, (128, toks), 0)
    first = ids_ref[0:1, :] == expert
    second = ids_ref[1:2, :] == expert
    member = jnp.where(first | second, 1.0, 0.0).astype(F32)
    weight_t = jnp.where(first, rw_ref[0:1, :], jnp.where(second, rw_ref[1:2, :], 0.0))
    upper = lax.broadcasted_iota(jnp.int32, (toks, toks), 0) < lax.broadcasted_iota(
        jnp.int32, (toks, toks), 1
    )
    upper = jnp.where(upper, 1.0, 0.0).astype(BF16)
    rank_t = jnp.dot(member.astype(BF16), upper, preferred_element_type=F32)
    place_t = jnp.where(member > 0.5, rank_t, -1.0)
    row_in = lax.broadcasted_iota(jnp.int32, (slot, toks), 0).astype(F32)
    slot_weight = []
    for e in range(n):
        hit = jnp.where(place_t[e : e + 1] == row_in, 1.0, 0.0).astype(F32)
        picks[e * slot : (e + 1) * slot, :] = hit.astype(BF16)
        slot_weight.append(jnp.sum(hit * weight_t[e : e + 1], 1, keepdims=True))
    slot_weight = jnp.concatenate(slot_weight, 0)
    for load in loads:
        load.wait()
    got = jnp.dot(picks[...], tok_part[...], preferred_element_type=F32).astype(BF16)
    send[:, 0] = got.reshape(n, slot, cols)
    got = jnp.dot(picks[...], og_part[...], preferred_element_type=F32)
    send[:, 1] = (got * slot_weight).astype(BF16).reshape(n, slot, cols)
    for j in range(2):
        rows[j, me, :, span(p, cols)] = send[me, j]
    pl.semaphore_wait(barrier, n + t - 2)

    def chunk(s, q):
        return rows.at[:, s, pl.ds(0, cap), span(q, cols)]

    def dispatch(i):
        return copy(
            send.at[ahead(i), :, pl.ds(0, cap), :], chunk(me, p), d_s.at[i], d_r.at[i],
            {"ep": ahead(i)},
        )

    def to_mirror(i):
        s = behind(i)
        return copy(chunk(s, p), chunk(s, p), m_s.at[i], m_r.at[i], {"tp": mirror})

    def to_buddy(i):
        s = behind(i)
        return copy(chunk(s, p), chunk(s, p), c_s.at[0, i], c_r.at[0, i], {"tp": buddy})

    def on_buddy(i):
        s = behind(i)
        return copy(
            chunk(s, mirror), chunk(s, mirror), c_s.at[1, i], c_r.at[1, i], {"tp": buddy}
        )

    def act_copy(i):
        return copy(act_send, act_all.at[:, me], a_s.at[i], a_r.at[i], {"ep": ahead(i)})

    def og_copy(i):
        return copy(
            og_send.at[ahead(i)], og_all.at[p, me], o_s.at[i], o_r.at[i], {"ep": ahead(i)}
        )

    def og_spread(i):
        return copy(og_all.at[p], og_all.at[p], q_s.at[i], q_r.at[i], {"tp": tp_ahead(i)})

    order = list(range(1, n))
    for i in order:
        dispatch(i).start()
    act_send[...] = act_part[...].reshape(t, part, sh)
    for e in range(n):
        og_send[e] = og_mine[:, e * cut : (e + 1) * cut]
    act_all[:, me] = act_send[...]
    og_all[p, me] = og_send[me]
    for i in range(n):
        if i:
            dispatch(i).wait_recv()
        to_mirror(i).start()
        to_buddy(i).start()
        if i:
            to_mirror(i - 1).wait_recv()
            on_buddy(i - 1).start()
    to_mirror(n - 1).wait_recv()
    on_buddy(n - 1).start()
    for i in order:
        og_copy(i).start()
    for i in order:
        act_copy(i).start()
    for w in weights:
        w.wait()
    for i in range(n):
        to_buddy(i).wait_recv()
        on_buddy(i).wait_recv()

    x_in = rows[0].reshape(total, width)
    x_cot = rows[1].reshape(total, width)
    tile = min(hid, 256)

    def forward(f, inner):
        at = pl.ds(pl.multiple_of(f * tile, tile), tile)
        gate_pre = lax.dot_general(x_in, wg[at, :], NT, preferred_element_type=F32)
        up_pre = lax.dot_general(x_in, wu[at, :], NT, preferred_element_type=F32)
        hidden_grad = lax.dot_general(x_cot, wd[at, :], NT, preferred_element_type=F32)
        sig = jax.nn.sigmoid(gate_pre)
        silu = gate_pre * sig
        hidden = (silu * up_pre).astype(BF16).astype(F32)
        up_d = hidden_grad * silu
        gate_d = hidden_grad * up_pre * sig * (1.0 + gate_pre * (1.0 - sig))
        delta[0, :, at] = gate_d.astype(BF16)
        delta[1, :, at] = up_d.astype(BF16)
        turned[0, at, :] = gate_d.T.astype(BF16)
        turned[1, at, :] = up_d.T.astype(BF16)
        turned[2, at, :] = hidden.T.astype(BF16)
        return inner + jnp.sum(hidden * hidden_grad, 1, keepdims=True)

    inner = lax.fori_loop(0, hid // tile, forward, jnp.zeros((total, 1), F32))
    inner_tp[p] = column_to_row(inner)

    def inner_copy(i):
        return copy(inner_tp.at[p], inner_tp.at[p], i_s.at[i], i_r.at[i], {"tp": tp_ahead(i)})

    for i in range(1, t):
        inner_copy(i).start()

    def share(q):
        at = span(q, cols)
        value = jnp.dot(delta[0], wg[:, at], preferred_element_type=F32)
        return value + jnp.dot(delta[1], wu[:, at], preferred_element_type=F32)

    def pair_copy(k):
        return copy(pair_send.at[k], pair_recv.at[k], p_s.at[k], p_r.at[k], {"tp": buddy})

    pair_send[0] = share(mirror_buddy).astype(BF16)
    pair_copy(0).start()
    acc_far[...] = share(mirror)
    pair_send[1] = share(buddy).astype(BF16)
    pair_copy(1).start()

    def far_copy(i):
        s = behind(i)
        return copy(far_send.at[s], far_recv.at[s], f_s.at[i], f_r.at[i], {"tp": mirror})

    pair_copy(0).wait_recv()
    far = acc_far[...] + pair_recv[0].astype(F32)
    far_send[...] = far.astype(BF16).reshape(n, slot, cols)
    back_order = list(range(1, n)) + [0]
    for i in back_order:
        far_copy(i).start()
    acc_own[...] = share(p).reshape(n, slot, cols)
    pair_copy(1).wait_recv()
    acc_own[...] = acc_own[...] + pair_recv[1].astype(F32).reshape(n, slot, cols)

    for i in range(1, t):
        inner_copy(i).wait_recv()
    inner_tot[...] = jnp.sum(inner_tp[...], 0)
    inner_ep[me] = inner_tot[...]

    def inner_back(i):
        return copy(inner_tot, inner_ep.at[me], j_s.at[i], j_r.at[i], {"ep": ahead(i)})

    for i in range(1, n):
        inner_back(i).start()

    def back_copy(i):
        return copy(
            back_send.at[behind(i), pl.ds(0, cap), :], back_recv.at[me, pl.ds(0, cap), :],
            b_s.at[i], b_r.at[i], {"ep": behind(i)},
        )

    if slot != cap:
        back_recv[:, cap:, :] = jnp.zeros((n, slot - cap, cols), BF16)
    for i in back_order:
        s = behind(i)
        far_copy(i).wait_recv()
        value = (acc_own[s] + far_recv[s].astype(F32)).astype(BF16)
        if i:
            back_send[s] = value
            back_copy(i).start()
        else:
            back_recv[me, 0:cap, :] = value[0:cap]

    for i in range(1, n):
        og_copy(i).wait_recv()
    for i in range(1, t):
        og_spread(i).start()
    for i in range(1, n):
        act_copy(i).wait_recv()

    block = min(width, 256)

    def grad_of(j, source):
        squares[...] = jnp.zeros_like(squares)

        def step(c, carry):
            at = pl.ds(pl.multiple_of(c * block, block), block)
            value = jnp.dot(
                turned[j], rows[source, :, :, at].reshape(total, block),
                preferred_element_type=F32,
            )
            (gate_out, up_out, down_out)[j][:, at] = value.astype(BF16)
            sq = value * value
            here = squares[...]
            for k in range(block // 128):
                here = here + sq[:, k * 128 : (k + 1) * 128]
            squares[...] = here
            return carry

        lax.fori_loop(0, width // block, step, 0)
        norms_out[j] = column_to_row(jnp.sum(squares[...], 1, keepdims=True))

    grad_of(0, 0)
    for i in range(1, t):
        og_spread(i).wait_recv()
    shared = lax.dot_general(
        act_all[...].reshape(n * toks, sh), og_all[...].reshape(n * toks, cut),
        (((0,), (0,)), ((), ())), preferred_element_type=F32,
    )
    shared_out[...] = shared
    snorm_all[me] = column_to_row(jnp.sum(shared * shared, 1, keepdims=True))

    def snorm_copy(i):
        return copy(
            snorm_all.at[me], snorm_all.at[me], n_s.at[i], n_r.at[i], {"ep": ahead(i)}
        )

    for i in range(1, n):
        snorm_copy(i).start()
    grad_of(1, 0)
    grad_of(2, 1)

    for i in range(1, n):
        inner_back(i).wait_recv()
    at_lane = lax.broadcasted_iota(jnp.int32, (toks, total), 1).astype(F32)
    base = (me * slot).astype(F32)
    rank = place_t.T
    found = jnp.zeros((toks, 128), F32)
    column = lax.broadcasted_iota(jnp.int32, (toks, 128), 1)
    for e in range(n):
        hit = at_lane == (rank[:, e : e + 1] + base)
        value = jnp.sum(jnp.where(hit, inner_ep[e], 0.0), 1, keepdims=True)
        found = jnp.where(column == e, value, found)
    found = found.T
    for k, chosen in enumerate((first, second)):
        value = jnp.sum(jnp.where(chosen, found, 0.0), 0, keepdims=True)
        route_out[k : k + 1, :] = value / rw_ref[k : k + 1, :]
    for i in range(1, n):
        back_copy(i).wait_recv()
    token_out[...] = lax.dot_general(
        picks[...], back_recv[...].reshape(total, cols), (((0,), (0,)), ((), ())),
        preferred_element_type=F32,
    ).astype(BF16)
    for i in range(1, n):
        snorm_copy(i).wait_recv()
    snorm_out[...] = jnp.sum(snorm_all[...], 0)

    for i in range(1, n):
        dispatch(i).wait_send()
        og_copy(i).wait_send()
        act_copy(i).wait_send()
        inner_back(i).wait_send()
        back_copy(i).wait_send()
        snorm_copy(i).wait_send()
    for i in range(n):
        to_mirror(i).wait_send()
        to_buddy(i).wait_send()
        on_buddy(i).wait_send()
        far_copy(i).wait_send()
    for i in range(1, t):
        og_spread(i).wait_send()
        inner_copy(i).wait_send()
    pair_copy(0).wait_send()
    pair_copy(1).wait_send()


def hand_over(*refs):
    count = (len(refs) - 1) // 2
    sources, targets, sem = refs[:count], refs[count : 2 * count], refs[-1]
    moves = []
    for j in sorted(range(count), key=lambda j: sources[j].size):
        moves.append(pltpu.make_async_copy(sources[j], targets[j], sem.at[j]))
        moves[-1].start()
    for move in moves:
        move.wait()


def fused(tokens, out_grad, expert_ids, route_weights, gate_proj, up_proj, down_proj, shared_act):
    n = lax.axis_size("ep")
    t = lax.axis_size("tp")
    toks, width = tokens.shape
    experts = gate_proj.shape[0] * n
    cap = 5 * toks * expert_ids.shape[1] // (4 * experts)
    slot = -(-cap // 16) * 16
    hid = gate_proj.shape[1]
    cols = width // t
    sh = shared_act.shape[1] // t
    cut = width // n
    part = toks // t
    total = n * slot
    vmem = pl.BlockSpec(memory_space=pltpu.VMEM)
    hbm = pl.BlockSpec(memory_space=pl.ANY)
    dma = pltpu.SemaphoreType.DMA
    results = pl.pallas_call(
        functools.partial(kernel, n, t, cap, slot),
        out_shape=(
            pltpu.VMEM((toks, cols), BF16),
            pltpu.VMEM((2, toks), F32),
            pltpu.VMEM((hid, width), BF16),
            pltpu.VMEM((hid, width), BF16),
            pltpu.VMEM((hid, width), BF16),
            pltpu.VMEM((3, 1, hid), F32),
            pltpu.VMEM((sh, cut), F32),
            pltpu.VMEM((1, sh), F32),
        ),
        in_specs=[vmem] * 2 + [hbm] * 6,
        out_specs=(vmem,) * 8,
        scratch_shapes=[
            pltpu.VMEM((n, 2, slot, cols), BF16),
            pltpu.VMEM((2, n, slot, width), BF16),
            pltpu.VMEM((hid, width), BF16),
            pltpu.VMEM((hid, width), BF16),
            pltpu.VMEM((hid, width), BF16),
            pltpu.VMEM((total, toks), BF16),
            pltpu.VMEM((2, total, hid), BF16),
            pltpu.VMEM((3, hid, total), BF16),
            pltpu.VMEM((hid, 128), F32),
            pltpu.VMEM((2, total, cols), BF16),
            pltpu.VMEM((2, total, cols), BF16),
            pltpu.VMEM((total, cols), F32),
            pltpu.VMEM((n, slot, cols), F32),
            pltpu.VMEM((n, slot, cols), BF16),
            pltpu.VMEM((n, slot, cols), BF16),
            pltpu.VMEM((n, slot, cols), BF16),
            pltpu.VMEM((n, slot, cols), BF16),
            pltpu.VMEM((t, 1, total), F32),
            pltpu.VMEM((1, total), F32),
            pltpu.VMEM((n, 1, total), F32),
            pltpu.VMEM((t, part, sh), BF16),
            pltpu.VMEM((t, n, part, sh), BF16),
            pltpu.VMEM((n, part, cut), BF16),
            pltpu.VMEM((t, n, part, cut), BF16),
            pltpu.VMEM((n, 1, sh), F32),
            pltpu.VMEM((toks, cols), BF16),
            pltpu.VMEM((toks, cols), BF16),
            pltpu.VMEM((part, width), BF16),
            pltpu.VMEM((toks, sh), BF16),
            dma((4,)),
            dma((3,)),
            dma((n,)), dma((n,)), dma((n,)), dma((n,)), dma((2, n)), dma((2, n)),
            dma((n,)), dma((n,)), dma((n,)), dma((n,)), dma((t,)), dma((t,)),
            dma((2,)), dma((2,)), dma((n,)), dma((n,)), dma((n,)), dma((n,)),
            dma((t,)), dma((t,)), dma((n,)), dma((n,)), dma((n,)), dma((n,)),
        ],
        compiler_params=pltpu.CompilerParams(
            collective_id=0, has_side_effects=True, vmem_limit_bytes=36 * 1024 * 1024
        ),
    )(
        *[
            pltpu.with_memory_space_constraint(r, pltpu.HBM)
            for r in (
                expert_ids.T, route_weights.T, tokens, out_grad, shared_act, gate_proj, up_proj,
                down_proj,
            )
        ]
    )
    count = len(results)
    token_grad, route, gate, up, down, norms, shared, snorm = pl.pallas_call(
        hand_over,
        out_shape=[jax.ShapeDtypeStruct(r.shape, r.dtype) for r in results],
        in_specs=[vmem] * count,
        out_specs=[hbm] * count,
        scratch_shapes=[dma((count,))],
        compiler_params=pltpu.CompilerParams(vmem_limit_bytes=4 * 1024 * 1024),
    )(*[pltpu.with_memory_space_constraint(r, pltpu.VMEM) for r in results])
    return (
        token_grad, route.T, gate[None], up[None], down[None], norms.transpose(1, 0, 2), shared,
        snorm[0],
    )


def local(tokens, out_grad, expert_ids, route_weights, gate_proj, up_proj, down_proj, shared_act):
    n = lax.axis_size("ep")
    t = lax.axis_size("tp")
    toks, width = tokens.shape
    hid = gate_proj.shape[1]
    slot = -(-(5 * toks * expert_ids.shape[1] // (4 * n)) // 16) * 16
    fits = (
        gate_proj.shape[0] == 1 and expert_ids.shape[1] == 2 and t == 4 and n in (2, 4, 8, 16, 32, 64, 128)
        and toks % 128 == 0 and toks // t % 16 == 0 and width // t % 128 == 0
        and hid % 256 == 0 and n * slot % 128 == 0 and width // n % 128 == 0
        and shared_act.shape[1] // t % 128 == 0
    )
    body = fused if fits else plain
    return body(
        tokens, out_grad, expert_ids, route_weights, gate_proj, up_proj, down_proj, shared_act
    )


def solution(mesh):
    placed = (
        P("ep", None),
        P("ep", None),
        P("ep", None),
        P("ep", None),
        P("ep", "tp", None),
        P("ep", "tp", None),
        P("ep", "tp", None),
        P("ep", None),
    )
    return jax.shard_map(
        local,
        mesh=mesh,
        in_specs=placed,
        out_specs=(
            P("ep", "tp"),
            P("ep", None),
            P("ep", "tp", None),
            P("ep", "tp", None),
            P("ep", "tp", None),
            P("ep", None, "tp"),
            P("tp", "ep"),
            P("tp"),
        ),
        check_vma=False,
    )
```

```python
import functools

import jax
import jax.numpy as jnp
from jax import lax
from jax.experimental import pallas as pl
from jax.experimental.pallas import tpu as pltpu
from jax.sharding import PartitionSpec as P


def plain(tokens, out_grad, expert_ids, route_weights, gate_proj, up_proj, down_proj, shared_act):
    ep_count = lax.axis_size("ep")
    tp_count = lax.axis_size("tp")
    tok_count, model_width = tokens.shape
    top_count = expert_ids.shape[1]
    exp_local = gate_proj.shape[0]
    experts = exp_local * ep_count
    capacity = 5 * tok_count * top_count // (4 * experts)
    slot_count = experts * capacity
    assign = tok_count * top_count
    columns = model_width // tp_count
    offset = lax.axis_index("tp") * columns
    flat_expert = expert_ids.reshape(assign)
    onehot = (flat_expert[:, None] == jnp.arange(experts, dtype=jnp.int32)[None, :]).astype(
        jnp.float32
    )
    earlier = (jnp.arange(assign)[:, None] > jnp.arange(assign)[None, :]).astype(jnp.float32)
    counted = jnp.dot(earlier, onehot, precision=lax.Precision.HIGHEST)
    rank_in = jnp.sum(counted * onehot, 1).astype(jnp.int32)
    slot_id = flat_expert * capacity + rank_in
    picked = (jnp.arange(slot_count, dtype=jnp.int32)[:, None] == slot_id[None, :]).astype(
        jnp.float32
    )
    source_id = jnp.dot(
        picked, jnp.arange(assign, dtype=jnp.float32), precision=lax.Precision.HIGHEST
    ).astype(jnp.int32)
    filled = jnp.sum(picked, 1) > 0.5
    scaled = (
        (route_weights[:, :, None] * out_grad[:, None, :])
        .astype(jnp.bfloat16)
        .reshape(assign, model_width)
    )

    def slot_rows(source_rows, row_index):
        taken = jnp.take(source_rows, row_index, axis=0)
        return jnp.where(filled[:, None], taken, jnp.zeros((), source_rows.dtype))

    token_part = lax.dynamic_slice_in_dim(tokens, offset, columns, 1)
    scaled_part = lax.dynamic_slice_in_dim(scaled, offset, columns, 1)
    send_in = slot_rows(token_part, source_id // top_count).reshape(
        ep_count, exp_local, capacity, columns
    )
    send_cot = slot_rows(scaled_part, source_id).reshape(ep_count, exp_local, capacity, columns)
    part_in, part_cot = (
        lax.all_to_all(send_in, "ep", split_axis=0, concat_axis=2, tiled=True),
        lax.all_to_all(send_cot, "ep", split_axis=0, concat_axis=2, tiled=True),
    )
    joined_in, joined_cot = (
        lax.all_gather(part_in, "tp", axis=3, tiled=True),
        lax.all_gather(part_cot, "tp", axis=3, tiled=True),
    )
    rows_in = joined_in[0]
    rows_cot = joined_cot[0]
    gate_pre = jnp.einsum("erd,efd->erf", rows_in, gate_proj, preferred_element_type=jnp.float32)
    up_pre = jnp.einsum("erd,efd->erf", rows_in, up_proj, preferred_element_type=jnp.float32)
    sigmoid_a = jax.nn.sigmoid(gate_pre)
    silu_a = gate_pre * sigmoid_a
    hidden = (silu_a * up_pre).astype(jnp.bfloat16)
    hidden_grad = jnp.einsum(
        "erd,efd->erf", rows_cot, down_proj, preferred_element_type=jnp.float32
    )
    up_delta = (hidden_grad * silu_a).astype(jnp.bfloat16)
    gate_delta = (hidden_grad * up_pre * sigmoid_a * (1.0 + gate_pre * (1.0 - sigmoid_a))).astype(
        jnp.bfloat16
    )
    gate_full = jnp.einsum("erf,erd->efd", gate_delta, rows_in, preferred_element_type=jnp.float32)
    up_full = jnp.einsum("erf,erd->efd", up_delta, rows_in, preferred_element_type=jnp.float32)
    down_full = jnp.einsum("erf,erd->efd", hidden, rows_cot, preferred_element_type=jnp.float32)
    row_norms = jnp.stack(
        [
            jnp.sum(gate_full * gate_full, 2),
            jnp.sum(up_full * up_full, 2),
            jnp.sum(down_full * down_full, 2),
        ],
        axis=1,
    )
    row_total = rows_in.shape[1]
    partial_value = jnp.einsum(
        "erf,efd->erd", gate_delta, gate_proj, preferred_element_type=jnp.float32
    )
    partial_value = partial_value + jnp.einsum(
        "erf,efd->erd", up_delta, up_proj, preferred_element_type=jnp.float32
    )
    partials = partial_value.astype(jnp.bfloat16).reshape(exp_local, row_total, tp_count, columns)
    inner_part = jnp.sum(hidden.astype(jnp.float32) * hidden_grad, 2).astype(jnp.bfloat16)
    inner_parts = jnp.broadcast_to(inner_part[:, :, None], (exp_local, row_total, tp_count))
    received, received_inner = (
        lax.all_to_all(partials, "tp", split_axis=2, concat_axis=2, tiled=True),
        lax.all_to_all(inner_parts, "tp", split_axis=2, concat_axis=2, tiled=True),
    )
    slot_grad = jnp.sum(received.astype(jnp.float32), 2)
    inner = jnp.sum(received_inner.astype(jnp.float32), 2)
    returned, returned_inner = (
        lax.all_to_all(
            slot_grad.reshape(exp_local, ep_count, capacity, columns),
            "ep",
            split_axis=1,
            concat_axis=0,
            tiled=True,
        ),
        lax.all_to_all(
            inner.reshape(exp_local, ep_count, capacity),
            "ep",
            split_axis=1,
            concat_axis=0,
            tiled=True,
        ),
    )
    slot_back = returned.reshape(slot_count, columns)
    inner_back = returned_inner.reshape(slot_count)
    token_grad = jnp.take(slot_back, slot_id, axis=0).reshape(tok_count, top_count, columns).sum(1)
    route_grad = jnp.take(inner_back, slot_id).reshape(tok_count, top_count) / route_weights
    shared_rows = shared_act.shape[1] // tp_count
    shared_part = lax.dynamic_slice_in_dim(
        shared_act, lax.axis_index("tp") * shared_rows, shared_rows, 1
    )
    shared_term = lax.dot_general(
        shared_part, out_grad, (((0,), (0,)), ((), ())), preferred_element_type=jnp.float32
    )
    shared_grad = lax.psum_scatter(shared_term, "ep", scatter_dimension=1, tiled=True)
    shared_norms = lax.psum(jnp.sum(shared_grad * shared_grad, 1), "ep")
    return (
        token_grad.astype(jnp.bfloat16),
        route_grad,
        gate_full.astype(jnp.bfloat16),
        up_full.astype(jnp.bfloat16),
        down_full.astype(jnp.bfloat16),
        row_norms,
        shared_grad,
        shared_norms,
    )


MESH = pl.DeviceIdType.MESH
F32 = jnp.float32
BF16 = jnp.bfloat16
NT = (((1,), (1,)), ((), ()))


def column_to_row(col, width=128):
    return jnp.broadcast_to(col, (col.shape[0], width)).T[0:1]


def kernel(
    n, t, cap, slot,
    ids_hbm, rw_hbm, tok_hbm, og_hbm, act_hbm, wg_hbm, wu_hbm, wd_hbm,
    token_out, route_out, gate_out, up_out, down_out, norms_out, shared_out, snorm_out,
    send, rows, wg, wu, wd, picks, place, weight_of, delta, turned, squares,
    pair_send, pair_recv, acc_far, acc_own, far_send, far_recv, back_send, back_recv,
    inner_tp, inner_tot, inner_ep, act_all, og_send, og_all, snorm_all,
    ids_ref, rw_ref, tok_part, og_part, tok_full, og_full, l_sem,
    w_sem, d_s, d_r, m_s, m_r, c_s, c_r, a_s, a_r, o_s, o_r, q_s, q_r,
    p_s, p_r, f_s, f_r, b_s, b_r, i_s, i_r, j_s, j_r, n_s, n_r,
):
    me = lax.axis_index("ep")
    p = lax.axis_index("tp")
    half = t // 2
    buddy = p + 1 - 2 * lax.rem(p, 2)
    mirror = lax.rem(p + half, t)
    mirror_buddy = lax.rem(buddy + half, t)
    toks, width = tok_hbm.shape
    cols = width // t
    hid = wg.shape[0]
    total = n * slot
    part = toks // 2
    core = lax.rem(p, 2)
    sh = act_hbm.shape[1] // t
    cut = width // n

    def span(q, size):
        return pl.ds(pl.multiple_of(q * size, 128), size)

    def peer(i):
        out, bit = 0, 1
        while bit < n:
            digit, flip = lax.rem(me // bit, 2), lax.rem(i // bit, 2)
            out = out + bit * (digit + flip - 2 * digit * flip)
            bit *= 2
        return out

    def tp_ahead(i):
        return lax.rem(p + i, t)

    def copy(src, dst, s_sem, r_sem, where):
        return pltpu.make_async_remote_copy(
            src_ref=src, dst_ref=dst, send_sem=s_sem, recv_sem=r_sem,
            device_id=where, device_id_type=MESH,
        )

    local = pltpu.make_async_copy
    loads = [
        local(tok_hbm.at[:, span(p, cols)], tok_part, l_sem.at[0]),
        local(og_hbm.at[:, span(p, cols)], og_part, l_sem.at[1]),
    ]
    own_loads = [
        local(tok_hbm, tok_full, l_sem.at[4]),
        local(og_hbm, og_full, l_sem.at[5]),
    ]
    late_loads = [
        local(
            act_hbm.at[q * part : (q + 1) * part, span(p, sh)], act_all.at[q, 0], l_sem.at[6 + q]
        )
        for q in range(2)
    ]
    for i in range(n):
        target = og_send.at[i] if i else og_all.at[core, 0]
        late_loads.append(
            local(
                og_hbm.at[pl.ds(pl.multiple_of(core * part, 16), part), span(peer(i), cut)],
                target, l_sem.at[8 + i],
            )
        )
    weights = [
        local(wg_hbm.at[0], wg, w_sem.at[0]),
        local(wu_hbm.at[0], wu, w_sem.at[1]),
        local(wd_hbm.at[0], wd, w_sem.at[2]),
    ]
    small_loads = [
        local(ids_hbm, ids_ref, l_sem.at[2]),
        local(rw_hbm, rw_ref, l_sem.at[3]),
    ]
    for load in small_loads + loads:
        load.start()
    barrier = pltpu.get_barrier_semaphore()
    for i in range(1, n):
        pl.semaphore_signal(barrier, inc=1, device_id={"ep": peer(i)}, device_id_type=MESH)
    for i in range(1, t):
        pl.semaphore_signal(barrier, inc=1, device_id={"tp": tp_ahead(i)}, device_id_type=MESH)
    for load in own_loads + weights + late_loads:
        load.start()

    for load in small_loads:
        load.wait()
    expert = lax.broadcasted_iota(jnp.int32, (128, toks), 0)
    first = ids_ref[0:1, :] == expert
    second = ids_ref[1:2, :] == expert
    member = jnp.where(first | second, 1.0, 0.0).astype(F32)
    weight_t = jnp.where(first, rw_ref[0:1, :], jnp.where(second, rw_ref[1:2, :], 0.0))
    upper = lax.broadcasted_iota(jnp.int32, (toks, toks), 0) < lax.broadcasted_iota(
        jnp.int32, (toks, toks), 1
    )
    upper = jnp.where(upper, 1.0, 0.0).astype(BF16)
    rank_t = jnp.dot(member.astype(BF16), upper, preferred_element_type=F32)
    place_t = jnp.where(member > 0.5, rank_t, -1.0)
    place[...] = place_t
    weight_of[...] = weight_t
    row_in = lax.broadcasted_iota(jnp.int32, (slot, toks), 0).astype(F32)
    slot_weight = []
    for i in range(n):
        at = pl.ds(peer(i), 1)
        hit = jnp.where(place[at, :] == row_in, 1.0, 0.0).astype(F32)
        picks[i * slot : (i + 1) * slot, :] = hit.astype(BF16)
        slot_weight.append(jnp.sum(hit * weight_of[at, :], 1, keepdims=True))
    for load in loads:
        load.wait()
    away = pl.ds(slot, total - slot)
    got = jnp.dot(picks[away, :], tok_part[...], preferred_element_type=F32).astype(BF16)
    send[1:, 0] = got.reshape(n - 1, slot, cols)
    got = jnp.dot(picks[away, :], og_part[...], preferred_element_type=F32)
    got = got * jnp.concatenate(slot_weight[1:], 0)
    send[1:, 1] = got.astype(BF16).reshape(n - 1, slot, cols)
    pl.semaphore_wait(barrier, n + t - 2)

    def chunk(i, q):
        return rows.at[:, i, pl.ds(0, cap), span(q, cols)]

    def dispatch(i):
        return copy(
            send.at[i, :, pl.ds(0, cap), :], chunk(i, p), d_s.at[i], d_r.at[i], {"ep": peer(i)}
        )

    def to_mirror(i):
        return copy(chunk(i, p), chunk(i, p), m_s.at[i], m_r.at[i], {"tp": mirror})

    def to_buddy(i):
        return copy(chunk(i, p), chunk(i, p), c_s.at[0, i], c_r.at[0, i], {"tp": buddy})

    def on_buddy(i):
        return copy(
            chunk(i, mirror), chunk(i, mirror), c_s.at[1, i], c_r.at[1, i], {"tp": buddy}
        )

    def act_copy(j):
        low = j & -j
        return copy(
            act_all.at[:, j - low], act_all.at[:, j], a_s.at[j], a_r.at[j], {"ep": peer(low)}
        )

    def act_from(j):
        bit = 1
        while bit < n and (j == 0 or bit < (j & -j)):
            act_copy(j + bit).start()
            bit *= 2

    def og_copy(i):
        return copy(og_send.at[i], og_all.at[core, i], o_s.at[i], o_r.at[i], {"ep": peer(i)})

    def og_buddy():
        return copy(og_all.at[core], og_all.at[core], q_s, q_r, {"tp": buddy})

    def inner_copy(i):
        return copy(inner_tp.at[p], inner_tp.at[p], i_s.at[i], i_r.at[i], {"tp": tp_ahead(i)})

    def inner_back(i):
        return copy(inner_tot, inner_ep.at[i], j_s.at[i], j_r.at[i], {"ep": peer(i)})

    def pair_copy(g, k):
        return copy(
            pair_send.at[g, k], pair_recv.at[g, k], p_s.at[g, k], p_r.at[g, k], {"tp": buddy}
        )

    def far_copy(i):
        at = pl.ds(0, cap)
        return copy(
            far_send.at[i, at, :], far_recv.at[i, at, :], f_s.at[i], f_r.at[i], {"tp": mirror}
        )

    def back_copy(i):
        at = pl.ds(0, cap)
        return copy(
            back_send.at[i, at, :], back_recv.at[i, at, :], b_s.at[i], b_r.at[i], {"ep": peer(i)}
        )

    def snorm_copy(i):
        return copy(snorm_all.at[0], snorm_all.at[i], n_s.at[i], n_r.at[i], {"ep": peer(i)})

    near = list(range(n // 2))
    distant = list(range(n // 2, n))
    groups = (near, distant)
    height = n // 2 * slot
    tile = min(hid, 256)

    for i in range(1, n):
        dispatch(i).start()
    for load in own_loads:
        load.wait()
    if slot != cap:
        rows[:, 1:, cap:, :] = jnp.zeros((2, n - 1, slot - cap, width), BF16)
        back_recv[:, cap:, :] = jnp.zeros((n, slot - cap, cols), BF16)
    rows[0, 0] = jnp.dot(picks[0:slot, :], tok_full[...], preferred_element_type=F32).astype(BF16)
    got = jnp.dot(picks[0:slot, :], og_full[...], preferred_element_type=F32)
    rows[1, 0] = (got * slot_weight[0]).astype(BF16)

    def pass_on(i):
        dispatch(i).wait_recv()
        to_mirror(i).start()
        to_buddy(i).start()

    def from_mirror(i):
        to_mirror(i).wait_recv()
        on_buddy(i).start()

    def settle(i):
        to_buddy(i).wait_recv()
        on_buddy(i).wait_recv()

    def forward(g, f):
        sources = slice(groups[g][0], groups[g][-1] + 1)
        at = slice(f * tile, (f + 1) * tile)
        x_in = rows[0, sources].reshape(height, width)
        x_cot = rows[1, sources].reshape(height, width)
        gate_pre = lax.dot_general(wg[at, :], x_in, NT, preferred_element_type=F32)
        up_pre = lax.dot_general(wu[at, :], x_in, NT, preferred_element_type=F32)
        hidden_grad = lax.dot_general(wd[at, :], x_cot, NT, preferred_element_type=F32)
        sig = jax.nn.sigmoid(gate_pre)
        silu = gate_pre * sig
        hidden = (silu * up_pre).astype(BF16)
        up_d = (hidden_grad * silu).astype(BF16)
        gate_d = (hidden_grad * up_pre * sig * (1.0 + gate_pre * (1.0 - sig))).astype(BF16)
        turned[g, 0, at, :] = gate_d
        turned[g, 1, at, :] = up_d
        turned[g, 2, at, :] = hidden
        delta[g, 0, :, at] = gate_d.T
        delta[g, 1, :, at] = up_d.T
        part_inner = jnp.sum(hidden.astype(F32) * hidden_grad, 0, keepdims=True)
        inner_tp[p, g] = part_inner if f == 0 else inner_tp[p, g] + part_inner

    def share(g, q):
        at = span(q, cols)
        value = jnp.dot(delta[g, 0], wg[:, at], preferred_element_type=F32)
        return value + jnp.dot(delta[g, 1], wu[:, at], preferred_element_type=F32)

    def shares_far(g):
        pair_send[g, 0] = share(g, mirror_buddy).astype(BF16)
        pair_copy(g, 0).start()
        acc_far[...] = share(g, mirror)
        pair_send[g, 1] = share(g, buddy).astype(BF16)
        pair_copy(g, 1).start()
        pair_copy(g, 0).wait_recv()
        far = (acc_far[...] + pair_recv[g, 0].astype(F32)).astype(BF16)
        far_send[groups[g][0] : groups[g][-1] + 1] = far.reshape(n // 2, slot, cols)

    def far_start(g):
        for i in order[g]:
            far_copy(i).start()

    def shares_own(g):
        value = share(g, p)
        pair_copy(g, 1).wait_recv()
        value = value + pair_recv[g, 1].astype(F32)
        acc_own[groups[g][0] : groups[g][-1] + 1] = value.reshape(n // 2, slot, cols)

    def give_back(i):
        far_copy(i).wait_recv()
        value = (acc_own[i, 0:cap] + far_recv[i, 0:cap].astype(F32)).astype(BF16)
        if isinstance(i, int) and i == 0:
            back_recv[0, 0:cap] = value
        else:
            back_send[i, 0:cap] = value
            back_copy(i).start()

    order = (near[1:] + near[:1], distant)
    steps = hid // tile

    ahead = near[1:] + distant[:1]
    for i in ahead:
        pass_on(i)
    for i in near[1:]:
        from_mirror(i)
    for w in weights:
        w.wait()
    for i in near[1:]:
        settle(i)
    rest = distant[1:]
    tiles = [f for f in range(steps)]
    for k, i in enumerate(rest):
        pass_on(i)
        if k == len(rest) - 1:
            count = len(tiles)
        else:
            count = max(1, steps // (len(rest) - 1))
        for f in tiles[:count]:
            forward(0, f)
        del tiles[:count]
        from_mirror(distant[k])
    for load in late_loads:
        load.wait()
    act_from(0)
    for j in distant + near[1:]:
        og_copy(j).start()
    shares_far(0)
    from_mirror(distant[-1])
    far_start(0)
    shares_own(0)
    for i in distant:
        settle(i)

    for f in range(steps):
        forward(1, f)
    for i in range(1, t):
        inner_copy(i).start()
    shares_far(1)
    far_start(1)
    levels = [1 << k for k in reversed(range(n.bit_length() - 1))]

    def act_level(low):
        for j in range(low, n, 2 * low):
            act_copy(j).wait_recv()
            act_from(j)

    act_level(levels[0])
    middle = [j for low in levels[1:-1] for j in range(low, n, 2 * low)]

    def act_next(count):
        for j in middle[:count]:
            act_copy(j).wait_recv()
            act_from(j)
        del middle[:count]

    act_next(1)
    for i in order[0]:
        give_back(i)
    shares_own(1)

    block = min(width, 512)
    chunks = width // block

    def grad_of(j, lo, hi):
        out = (gate_out, up_out, down_out)[j]
        source = j // 2

        def step(c, carry):
            at = pl.ds(pl.multiple_of(c * block, block), block)
            value = jnp.dot(
                turned[0, j], rows[source, 0 : n // 2, :, at].reshape(height, block),
                preferred_element_type=F32,
            )
            value = value + jnp.dot(
                turned[1, j], rows[source, n // 2 :, :, at].reshape(height, block),
                preferred_element_type=F32,
            )
            out[:, at] = value.astype(BF16)
            sq = value * value
            here = squares[j]
            for k in range(block // 128):
                here = here + sq[:, k * 128 : (k + 1) * 128]
            squares[j] = here
            return carry

        lax.fori_loop(lo, hi, step, 0)

    squares[...] = jnp.zeros_like(squares)
    todo = [(j, c) for j in range(3) for c in range(chunks)]

    def spend(count):
        for j, c in todo[:count]:
            grad_of(j, c, c + 1)
        del todo[:count]

    for i in range(1, t):
        inner_copy(i).wait_recv()
    inner_tot[...] = jnp.sum(inner_tp[...], 0)
    inner_ep[0] = inner_tot[...]
    for i in range(1, n):
        inner_back(i).start()
    for k, i in enumerate(order[1]):
        spend(1)
        give_back(i)
        if k:
            act_next(1)
    act_next(len(middle))
    spend(len(todo))
    for j in range(3):
        norms_out[j] = column_to_row(jnp.sum(squares[j], 1, keepdims=True))
    for i in range(1, n):
        og_copy(i).wait_recv()
    og_buddy().start()
    act_level(levels[-1])
    og_buddy().wait_recv()
    shared = lax.dot_general(
        act_all[...].reshape(n * toks, sh), og_all[...].reshape(n * toks, cut),
        (((0,), (0,)), ((), ())), preferred_element_type=F32,
    )
    shared_out[...] = shared
    snorm_all[0] = column_to_row(jnp.sum(shared * shared, 1, keepdims=True))
    for i in range(1, n):
        snorm_copy(i).start()
    for i in range(1, n):
        inner_back(i).wait_recv()
    found = jnp.zeros((n, toks), F32)
    for g in range(2):
        block_of = lax.broadcasted_iota(jnp.int32, (n, height), 1) // slot + g * n // 2
        row_of = lax.broadcasted_iota(jnp.int32, (n, height), 0)
        spread = jnp.zeros((n, height), F32)
        for i in groups[g]:
            spread = jnp.where((block_of == i) & (row_of == i), inner_ep[i, g], spread)
        found = found + jnp.dot(
            spread, picks[g * height : (g + 1) * height, :].astype(F32),
            precision=lax.Precision.HIGHEST, preferred_element_type=F32,
        )
    for k in range(2):
        value = jnp.zeros((1, toks), F32)
        for i in range(n):
            value = value + jnp.where(ids_ref[k : k + 1, :] == peer(i), found[i : i + 1], 0.0)
        route_out[k : k + 1, :] = value / rw_ref[k : k + 1, :]
    for i in range(1, n):
        back_copy(i).wait_recv()
    token_out[...] = lax.dot_general(
        picks[...], back_recv[...].reshape(total, cols), (((0,), (0,)), ((), ())),
        preferred_element_type=F32,
    ).astype(BF16)
    for i in range(1, n):
        snorm_copy(i).wait_recv()
    snorm_out[...] = jnp.sum(snorm_all[...], 0)

    for i in range(1, n):
        dispatch(i).wait_send()
        to_mirror(i).wait_send()
    for i in range(1, n):
        to_buddy(i).wait_send()
        on_buddy(i).wait_send()
        og_copy(i).wait_send()
        act_copy(i).wait_send()
        inner_back(i).wait_send()
        back_copy(i).wait_send()
        snorm_copy(i).wait_send()
    for i in range(n):
        far_copy(i).wait_send()
    for i in range(1, t):
        inner_copy(i).wait_send()
    og_buddy().wait_send()
    for g in range(2):
        for k in range(2):
            pair_copy(g, k).wait_send()


def hand_over(*refs):
    count = (len(refs) - 1) // 2
    sources, targets, sem = refs[:count], refs[count : 2 * count], refs[-1]
    moves = []
    for j in sorted(range(count), key=lambda j: sources[j].size):
        moves.append(pltpu.make_async_copy(sources[j], targets[j], sem.at[j]))
        moves[-1].start()
    for move in moves:
        move.wait()


def fused(tokens, out_grad, expert_ids, route_weights, gate_proj, up_proj, down_proj, shared_act):
    n = lax.axis_size("ep")
    t = lax.axis_size("tp")
    toks, width = tokens.shape
    experts = gate_proj.shape[0] * n
    cap = 5 * toks * expert_ids.shape[1] // (4 * experts)
    slot = -(-cap // 16) * 16
    hid = gate_proj.shape[1]
    cols = width // t
    sh = shared_act.shape[1] // t
    cut = width // n
    part = toks // 2
    total = n * slot
    height = total // 2
    vmem = pl.BlockSpec(memory_space=pltpu.VMEM)
    hbm = pl.BlockSpec(memory_space=pl.ANY)
    dma = pltpu.SemaphoreType.DMA
    results = pl.pallas_call(
        functools.partial(kernel, n, t, cap, slot),
        out_shape=(
            pltpu.VMEM((toks, cols), BF16),
            pltpu.VMEM((2, toks), F32),
            pltpu.VMEM((hid, width), BF16),
            pltpu.VMEM((hid, width), BF16),
            pltpu.VMEM((hid, width), BF16),
            pltpu.VMEM((3, 1, hid), F32),
            pltpu.VMEM((sh, cut), F32),
            pltpu.VMEM((1, sh), F32),
        ),
        in_specs=[hbm] * 8,
        out_specs=(vmem,) * 8,
        scratch_shapes=[
            pltpu.VMEM((n, 2, slot, cols), BF16),
            pltpu.VMEM((2, n, slot, width), BF16),
            pltpu.VMEM((hid, width), BF16),
            pltpu.VMEM((hid, width), BF16),
            pltpu.VMEM((hid, width), BF16),
            pltpu.VMEM((total, toks), BF16),
            pltpu.VMEM((128, toks), F32),
            pltpu.VMEM((128, toks), F32),
            pltpu.VMEM((2, 2, height, hid), BF16),
            pltpu.VMEM((2, 3, hid, height), BF16),
            pltpu.VMEM((3, hid, 128), F32),
            pltpu.VMEM((2, 2, height, cols), BF16),
            pltpu.VMEM((2, 2, height, cols), BF16),
            pltpu.VMEM((height, cols), F32),
            pltpu.VMEM((n, slot, cols), F32),
            pltpu.VMEM((n, slot, cols), BF16),
            pltpu.VMEM((n, slot, cols), BF16),
            pltpu.VMEM((n, slot, cols), BF16),
            pltpu.VMEM((n, slot, cols), BF16),
            pltpu.VMEM((t, 2, 1, height), F32),
            pltpu.VMEM((2, 1, height), F32),
            pltpu.VMEM((n, 2, 1, height), F32),
            pltpu.VMEM((2, n, part, sh), BF16),
            pltpu.VMEM((n, part, cut), BF16),
            pltpu.VMEM((2, n, part, cut), BF16),
            pltpu.VMEM((n, 1, sh), F32),
            pltpu.VMEM((2, toks), jnp.int32),
            pltpu.VMEM((2, toks), F32),
            pltpu.VMEM((toks, cols), BF16),
            pltpu.VMEM((toks, cols), BF16),
            pltpu.VMEM((toks, width), BF16),
            pltpu.VMEM((toks, width), BF16),
            dma((8 + n,)),
            dma((3,)),
            dma((n,)), dma((n,)), dma((n,)), dma((n,)), dma((2, n)), dma((2, n)),
            dma((n,)), dma((n,)), dma((n,)), dma((n,)), dma, dma,
            dma((2, 2)), dma((2, 2)), dma((n,)), dma((n,)), dma((n,)), dma((n,)),
            dma((t,)), dma((t,)), dma((n,)), dma((n,)), dma((n,)), dma((n,)),
        ],
        compiler_params=pltpu.CompilerParams(
            collective_id=0, has_side_effects=True, vmem_limit_bytes=36 * 1024 * 1024
        ),
    )(
        *[
            pltpu.with_memory_space_constraint(r, pltpu.HBM)
            for r in (
                expert_ids.T, route_weights.T, tokens, out_grad, shared_act, gate_proj, up_proj,
                down_proj,
            )
        ]
    )
    count = len(results)
    token_grad, route, gate, up, down, norms, shared, snorm = pl.pallas_call(
        hand_over,
        out_shape=[jax.ShapeDtypeStruct(r.shape, r.dtype) for r in results],
        in_specs=[vmem] * count,
        out_specs=[hbm] * count,
        scratch_shapes=[dma((count,))],
        compiler_params=pltpu.CompilerParams(vmem_limit_bytes=4 * 1024 * 1024),
    )(*[pltpu.with_memory_space_constraint(r, pltpu.VMEM) for r in results])
    return (
        token_grad, route.T, gate[None], up[None], down[None], norms.transpose(1, 0, 2), shared,
        snorm[0],
    )


def local(tokens, out_grad, expert_ids, route_weights, gate_proj, up_proj, down_proj, shared_act):
    n = lax.axis_size("ep")
    t = lax.axis_size("tp")
    toks, width = tokens.shape
    hid = gate_proj.shape[1]
    slot = -(-(5 * toks * expert_ids.shape[1] // (4 * n)) // 16) * 16
    fits = (
        gate_proj.shape[0] == 1 and expert_ids.shape[1] == 2 and t == 4 and n >= 8 and n & (n - 1) == 0 and n <= 128
        and toks % 128 == 0 and toks % 32 == 0 and width // t % 128 == 0
        and hid % 512 == 0 and n * slot % 128 == 0 and width // n % 128 == 0
        and shared_act.shape[1] // t % 128 == 0
    )
    body = fused if fits else plain
    return body(
        tokens, out_grad, expert_ids, route_weights, gate_proj, up_proj, down_proj, shared_act
    )


def solution(mesh):
    placed = (
        P("ep", None),
        P("ep", None),
        P("ep", None),
        P("ep", None),
        P("ep", "tp", None),
        P("ep", "tp", None),
        P("ep", "tp", None),
        P("ep", None),
    )
    return jax.shard_map(
        local,
        mesh=mesh,
        in_specs=placed,
        out_specs=(
            P("ep", "tp"),
            P("ep", None),
            P("ep", "tp", None),
            P("ep", "tp", None),
            P("ep", "tp", None),
            P("ep", None, "tp"),
            P("tp", "ep"),
            P("tp"),
        ),
        check_vma=False,
    )
```

```python
import functools

import jax
import jax.numpy as jnp
from jax import lax
from jax.experimental import pallas as pl
from jax.experimental.pallas import tpu as pltpu
from jax.sharding import PartitionSpec as P


def plain(tokens, out_grad, expert_ids, route_weights, gate_proj, up_proj, down_proj, shared_act):
    ep_count = lax.axis_size("ep")
    tp_count = lax.axis_size("tp")
    tok_count, model_width = tokens.shape
    top_count = expert_ids.shape[1]
    exp_local = gate_proj.shape[0]
    experts = exp_local * ep_count
    capacity = 5 * tok_count * top_count // (4 * experts)
    slot_count = experts * capacity
    assign = tok_count * top_count
    columns = model_width // tp_count
    offset = lax.axis_index("tp") * columns
    flat_expert = expert_ids.reshape(assign)
    onehot = (flat_expert[:, None] == jnp.arange(experts, dtype=jnp.int32)[None, :]).astype(
        jnp.float32
    )
    earlier = (jnp.arange(assign)[:, None] > jnp.arange(assign)[None, :]).astype(jnp.float32)
    counted = jnp.dot(earlier, onehot, precision=lax.Precision.HIGHEST)
    rank_in = jnp.sum(counted * onehot, 1).astype(jnp.int32)
    slot_id = flat_expert * capacity + rank_in
    picked = (jnp.arange(slot_count, dtype=jnp.int32)[:, None] == slot_id[None, :]).astype(
        jnp.float32
    )
    source_id = jnp.dot(
        picked, jnp.arange(assign, dtype=jnp.float32), precision=lax.Precision.HIGHEST
    ).astype(jnp.int32)
    filled = jnp.sum(picked, 1) > 0.5
    scaled = (
        (route_weights[:, :, None] * out_grad[:, None, :])
        .astype(jnp.bfloat16)
        .reshape(assign, model_width)
    )

    def slot_rows(source_rows, row_index):
        taken = jnp.take(source_rows, row_index, axis=0)
        return jnp.where(filled[:, None], taken, jnp.zeros((), source_rows.dtype))

    token_part = lax.dynamic_slice_in_dim(tokens, offset, columns, 1)
    scaled_part = lax.dynamic_slice_in_dim(scaled, offset, columns, 1)
    send_in = slot_rows(token_part, source_id // top_count).reshape(
        ep_count, exp_local, capacity, columns
    )
    send_cot = slot_rows(scaled_part, source_id).reshape(ep_count, exp_local, capacity, columns)
    part_in, part_cot = (
        lax.all_to_all(send_in, "ep", split_axis=0, concat_axis=2, tiled=True),
        lax.all_to_all(send_cot, "ep", split_axis=0, concat_axis=2, tiled=True),
    )
    joined_in, joined_cot = (
        lax.all_gather(part_in, "tp", axis=3, tiled=True),
        lax.all_gather(part_cot, "tp", axis=3, tiled=True),
    )
    rows_in = joined_in[0]
    rows_cot = joined_cot[0]
    gate_pre = jnp.einsum("erd,efd->erf", rows_in, gate_proj, preferred_element_type=jnp.float32)
    up_pre = jnp.einsum("erd,efd->erf", rows_in, up_proj, preferred_element_type=jnp.float32)
    sigmoid_a = jax.nn.sigmoid(gate_pre)
    silu_a = gate_pre * sigmoid_a
    hidden = (silu_a * up_pre).astype(jnp.bfloat16)
    hidden_grad = jnp.einsum(
        "erd,efd->erf", rows_cot, down_proj, preferred_element_type=jnp.float32
    )
    up_delta = (hidden_grad * silu_a).astype(jnp.bfloat16)
    gate_delta = (hidden_grad * up_pre * sigmoid_a * (1.0 + gate_pre * (1.0 - sigmoid_a))).astype(
        jnp.bfloat16
    )
    gate_full = jnp.einsum("erf,erd->efd", gate_delta, rows_in, preferred_element_type=jnp.float32)
    up_full = jnp.einsum("erf,erd->efd", up_delta, rows_in, preferred_element_type=jnp.float32)
    down_full = jnp.einsum("erf,erd->efd", hidden, rows_cot, preferred_element_type=jnp.float32)
    row_norms = jnp.stack(
        [
            jnp.sum(gate_full * gate_full, 2),
            jnp.sum(up_full * up_full, 2),
            jnp.sum(down_full * down_full, 2),
        ],
        axis=1,
    )
    row_total = rows_in.shape[1]
    partial_value = jnp.einsum(
        "erf,efd->erd", gate_delta, gate_proj, preferred_element_type=jnp.float32
    )
    partial_value = partial_value + jnp.einsum(
        "erf,efd->erd", up_delta, up_proj, preferred_element_type=jnp.float32
    )
    partials = partial_value.astype(jnp.bfloat16).reshape(exp_local, row_total, tp_count, columns)
    inner_part = jnp.sum(hidden.astype(jnp.float32) * hidden_grad, 2).astype(jnp.bfloat16)
    inner_parts = jnp.broadcast_to(inner_part[:, :, None], (exp_local, row_total, tp_count))
    received, received_inner = (
        lax.all_to_all(partials, "tp", split_axis=2, concat_axis=2, tiled=True),
        lax.all_to_all(inner_parts, "tp", split_axis=2, concat_axis=2, tiled=True),
    )
    slot_grad = jnp.sum(received.astype(jnp.float32), 2)
    inner = jnp.sum(received_inner.astype(jnp.float32), 2)
    returned, returned_inner = (
        lax.all_to_all(
            slot_grad.reshape(exp_local, ep_count, capacity, columns),
            "ep",
            split_axis=1,
            concat_axis=0,
            tiled=True,
        ),
        lax.all_to_all(
            inner.reshape(exp_local, ep_count, capacity),
            "ep",
            split_axis=1,
            concat_axis=0,
            tiled=True,
        ),
    )
    slot_back = returned.reshape(slot_count, columns)
    inner_back = returned_inner.reshape(slot_count)
    token_grad = jnp.take(slot_back, slot_id, axis=0).reshape(tok_count, top_count, columns).sum(1)
    route_grad = jnp.take(inner_back, slot_id).reshape(tok_count, top_count) / route_weights
    shared_rows = shared_act.shape[1] // tp_count
    shared_part = lax.dynamic_slice_in_dim(
        shared_act, lax.axis_index("tp") * shared_rows, shared_rows, 1
    )
    shared_term = lax.dot_general(
        shared_part, out_grad, (((0,), (0,)), ((), ())), preferred_element_type=jnp.float32
    )
    shared_grad = lax.psum_scatter(shared_term, "ep", scatter_dimension=1, tiled=True)
    shared_norms = lax.psum(jnp.sum(shared_grad * shared_grad, 1), "ep")
    return (
        token_grad.astype(jnp.bfloat16),
        route_grad,
        gate_full.astype(jnp.bfloat16),
        up_full.astype(jnp.bfloat16),
        down_full.astype(jnp.bfloat16),
        row_norms,
        shared_grad,
        shared_norms,
    )


MESH = pl.DeviceIdType.MESH
F32 = jnp.float32
BF16 = jnp.bfloat16
NT = (((1,), (1,)), ((), ()))


def column_to_row(col, width=128):
    return jnp.broadcast_to(col, (col.shape[0], width)).T[0:1]


def kernel(
    n, t, cap, slot,
    ids_hbm, rw_hbm, tok_hbm, og_hbm, act_hbm, wg_hbm, wu_hbm, wd_hbm,
    token_out, route_out, gate_out, up_out, down_out, norms_out, shared_out, snorm_out,
    send, rows, wg, wu, wd, picks, place, weight_of, delta_a, delta_b, turned_a, turned_b, squares,
    pair_send, pair_recv, acc_far, acc_own, far_send, far_recv, back_send, back_recv,
    inner_tp, inner_tot, inner_ep, act_all, og_send, og_all, snorm_all,
    ids_ref, rw_ref, tok_part, og_part, tok_full, og_full, l_sem,
    w_sem, d_s, d_r, m_s, m_r, c_s, c_r, a_s, a_r, o_s, o_r, q_s, q_r,
    p_s, p_r, f_s, f_r, b_s, b_r, i_s, i_r, j_s, j_r, n_s, n_r,
):
    me = lax.axis_index("ep")
    p = lax.axis_index("tp")
    half = t // 2
    buddy = p + 1 - 2 * lax.rem(p, 2)
    mirror = lax.rem(p + half, t)
    mirror_buddy = lax.rem(buddy + half, t)
    toks, width = tok_hbm.shape
    cols = width // t
    hid = wg.shape[0]
    total = n * slot
    part = toks // 2
    core = lax.rem(p, 2)
    sh = act_hbm.shape[1] // t
    cut = width // n

    def span(q, size):
        return pl.ds(pl.multiple_of(q * size, 128), size)

    def peer(i):
        out, bit = 0, 1
        while bit < n:
            digit, flip = lax.rem(me // bit, 2), lax.rem(i // bit, 2)
            out = out + bit * (digit + flip - 2 * digit * flip)
            bit *= 2
        return out

    def tp_ahead(i):
        return lax.rem(p + i, t)

    def copy(src, dst, s_sem, r_sem, where):
        return pltpu.make_async_remote_copy(
            src_ref=src, dst_ref=dst, send_sem=s_sem, recv_sem=r_sem,
            device_id=where, device_id_type=MESH,
        )

    near = list(range(n // 2 + 1))
    distant = list(range(n // 2 + 1, n))
    groups = (near, distant)
    heights = [len(group) * slot for group in groups]
    delta, turned = (delta_a, delta_b), (turned_a, turned_b)
    local = pltpu.make_async_copy
    loads = [
        local(tok_hbm.at[:, span(p, cols)], tok_part, l_sem.at[0]),
        local(og_hbm.at[:, span(p, cols)], og_part, l_sem.at[1]),
    ]
    own_loads = [
        local(tok_hbm, tok_full, l_sem.at[4]),
        local(og_hbm, og_full, l_sem.at[5]),
    ]
    late_loads = [
        local(
            act_hbm.at[q * part : (q + 1) * part, span(p, sh)], act_all.at[q, 0], l_sem.at[6 + q]
        )
        for q in range(2)
    ]
    for i in range(n):
        target = og_send.at[i] if i else og_all.at[core, 0]
        late_loads.append(
            local(
                og_hbm.at[pl.ds(pl.multiple_of(core * part, 16), part), span(peer(i), cut)],
                target, l_sem.at[8 + i],
            )
        )
    weights = [
        local(wg_hbm.at[0], wg, w_sem.at[0]),
        local(wu_hbm.at[0], wu, w_sem.at[1]),
        local(wd_hbm.at[0], wd, w_sem.at[2]),
    ]
    small_loads = [
        local(ids_hbm, ids_ref, l_sem.at[2]),
        local(rw_hbm, rw_ref, l_sem.at[3]),
    ]
    for load in small_loads + loads:
        load.start()
    barrier = pltpu.get_barrier_semaphore()
    for i in range(1, n):
        pl.semaphore_signal(barrier, inc=1, device_id={"ep": peer(i)}, device_id_type=MESH)
    for i in range(1, t):
        pl.semaphore_signal(barrier, inc=1, device_id={"tp": tp_ahead(i)}, device_id_type=MESH)
    for load in own_loads + weights + late_loads:
        load.start()

    for load in small_loads:
        load.wait()
    expert = lax.broadcasted_iota(jnp.int32, (128, toks), 0)
    first = ids_ref[0:1, :] == expert
    second = ids_ref[1:2, :] == expert
    member = jnp.where(first | second, 1.0, 0.0).astype(F32)
    weight_t = jnp.where(first, rw_ref[0:1, :], jnp.where(second, rw_ref[1:2, :], 0.0))
    upper = lax.broadcasted_iota(jnp.int32, (toks, toks), 0) < lax.broadcasted_iota(
        jnp.int32, (toks, toks), 1
    )
    upper = jnp.where(upper, 1.0, 0.0).astype(BF16)
    rank_t = jnp.dot(member.astype(BF16), upper, preferred_element_type=F32)
    place_t = jnp.where(member > 0.5, rank_t, -1.0)
    place[...] = place_t
    weight_of[...] = weight_t
    row_in = lax.broadcasted_iota(jnp.int32, (slot, toks), 0).astype(F32)
    slot_weight = []
    for i in range(n):
        at = pl.ds(peer(i), 1)
        hit = jnp.where(place[at, :] == row_in, 1.0, 0.0).astype(F32)
        picks[i * slot : (i + 1) * slot, :] = hit.astype(BF16)
        slot_weight.append(jnp.sum(hit * weight_of[at, :], 1, keepdims=True))
    for load in loads:
        load.wait()
    away = pl.ds(slot, total - slot)
    got = jnp.dot(picks[away, :], tok_part[...], preferred_element_type=F32).astype(BF16)
    send[1:, 0] = got.reshape(n - 1, slot, cols)
    got = jnp.dot(picks[away, :], og_part[...], preferred_element_type=F32)
    got = got * jnp.concatenate(slot_weight[1:], 0)
    send[1:, 1] = got.astype(BF16).reshape(n - 1, slot, cols)
    pl.semaphore_wait(barrier, n + t - 2)

    def chunk(i, q):
        return rows.at[:, i, pl.ds(0, cap), span(q, cols)]

    def dispatch(i):
        return copy(
            send.at[i, :, pl.ds(0, cap), :], chunk(i, p), d_s.at[i], d_r.at[i], {"ep": peer(i)}
        )

    def to_mirror(i):
        return copy(chunk(i, p), chunk(i, p), m_s.at[i], m_r.at[i], {"tp": mirror})

    def to_buddy(i):
        return copy(chunk(i, p), chunk(i, p), c_s.at[0, i], c_r.at[0, i], {"tp": buddy})

    def on_buddy(i):
        return copy(
            chunk(i, mirror), chunk(i, mirror), c_s.at[1, i], c_r.at[1, i], {"tp": buddy}
        )

    def act_copy(j):
        low = j & -j
        return copy(
            act_all.at[:, j - low], act_all.at[:, j], a_s.at[j], a_r.at[j], {"ep": peer(low)}
        )

    def act_from(j):
        bit = (n if j == 0 else j & -j) // 2
        while bit:
            act_copy(j + bit).start()
            bit //= 2

    def og_copy(i):
        return copy(og_send.at[i], og_all.at[core, i], o_s.at[i], o_r.at[i], {"ep": peer(i)})

    def og_buddy():
        return copy(og_all.at[core], og_all.at[core], q_s, q_r, {"tp": buddy})

    def inner_copy(i):
        return copy(inner_tp.at[p], inner_tp.at[p], i_s.at[i], i_r.at[i], {"tp": tp_ahead(i)})

    def inner_back(i):
        return copy(inner_tot, inner_ep.at[i], j_s.at[i], j_r.at[i], {"ep": peer(i)})

    def pair_copy(g, k):
        at = pl.ds(0, heights[g])
        return copy(
            pair_send.at[g, k, at, :], pair_recv.at[g, k, at, :], p_s.at[g, k], p_r.at[g, k],
            {"tp": buddy},
        )

    def far_copy(i):
        at = pl.ds(0, cap)
        return copy(
            far_send.at[i, at, :], far_recv.at[i, at, :], f_s.at[i], f_r.at[i], {"tp": mirror}
        )

    def back_copy(i):
        at = pl.ds(0, cap)
        return copy(
            back_send.at[i, at, :], back_recv.at[i, at, :], b_s.at[i], b_r.at[i], {"ep": peer(i)}
        )

    def snorm_copy(i):
        return copy(snorm_all.at[0], snorm_all.at[i], n_s.at[i], n_r.at[i], {"ep": peer(i)})

    tile = min(hid, 256)

    for i in range(1, n):
        dispatch(i).start()
    for load in own_loads:
        load.wait()
    inner_tp[p] = jnp.zeros_like(inner_tp[p])
    if slot != cap:
        rows[:, 1:, cap:, :] = jnp.zeros((2, n - 1, slot - cap, width), BF16)
        back_recv[:, cap:, :] = jnp.zeros((n, slot - cap, cols), BF16)
    rows[0, 0] = jnp.dot(picks[0:slot, :], tok_full[...], preferred_element_type=F32).astype(BF16)
    got = jnp.dot(picks[0:slot, :], og_full[...], preferred_element_type=F32)
    rows[1, 0] = (got * slot_weight[0]).astype(BF16)

    def pass_on(i):
        dispatch(i).wait_recv()
        to_mirror(i).start()
        to_buddy(i).start()

    def from_mirror(i):
        to_mirror(i).wait_recv()
        on_buddy(i).start()

    def settle(i):
        to_buddy(i).wait_recv()
        on_buddy(i).wait_recv()

    def forward(g, f):
        sources = slice(groups[g][0], groups[g][-1] + 1)
        at = slice(f * tile, (f + 1) * tile)
        x_in = rows[0, sources].reshape(heights[g], width)
        x_cot = rows[1, sources].reshape(heights[g], width)
        gate_pre = lax.dot_general(wg[at, :], x_in, NT, preferred_element_type=F32)
        up_pre = lax.dot_general(wu[at, :], x_in, NT, preferred_element_type=F32)
        hidden_grad = lax.dot_general(wd[at, :], x_cot, NT, preferred_element_type=F32)
        sig = jax.nn.sigmoid(gate_pre)
        silu = gate_pre * sig
        hidden = (silu * up_pre).astype(BF16)
        up_d = (hidden_grad * silu).astype(BF16)
        gate_d = (hidden_grad * up_pre * sig * (1.0 + gate_pre * (1.0 - sig))).astype(BF16)
        turned[g][0, at, :] = gate_d
        turned[g][1, at, :] = up_d
        turned[g][2, at, :] = hidden
        delta[g][0, :, at] = gate_d.T
        delta[g][1, :, at] = up_d.T
        part_inner = jnp.sum(hidden.astype(F32) * hidden_grad, 0, keepdims=True)
        if f:
            part_inner = part_inner + inner_tp[p, g, :, 0 : heights[g]]
        inner_tp[p, g, :, 0 : heights[g]] = part_inner

    def share(g, q):
        at = span(q, cols)
        value = jnp.dot(delta[g][0], wg[:, at], preferred_element_type=F32)
        return value + jnp.dot(delta[g][1], wu[:, at], preferred_element_type=F32)

    def shares_far(g, between=None):
        own = pl.ds(0, heights[g])
        pair_send[g, 0, own] = share(g, mirror_buddy).astype(BF16)
        pair_copy(g, 0).start()
        acc_far[own] = share(g, mirror)
        pair_send[g, 1, own] = share(g, buddy).astype(BF16)
        pair_copy(g, 1).start()
        if between:
            between()
        pair_copy(g, 0).wait_recv()
        far = (acc_far[own] + pair_recv[g, 0, own].astype(F32)).astype(BF16)
        far_send[groups[g][0] : groups[g][-1] + 1] = far.reshape(len(groups[g]), slot, cols)

    def far_start(g):
        for i in order[g]:
            far_copy(i).start()

    def shares_own(g):
        value = share(g, p)
        pair_copy(g, 1).wait_recv()
        value = value + pair_recv[g, 1, 0 : heights[g]].astype(F32)
        acc_own[groups[g][0] : groups[g][-1] + 1] = value.reshape(len(groups[g]), slot, cols)

    def give_back(i):
        far_copy(i).wait_recv()
        value = (acc_own[i, 0:cap] + far_recv[i, 0:cap].astype(F32)).astype(BF16)
        if isinstance(i, int) and i == 0:
            back_recv[0, 0:cap] = value
        else:
            back_send[i, 0:cap] = value
            back_copy(i).start()

    order = (near[-1:] + near[1:-1], distant)
    steps = hid // tile

    for i in near[1:]:
        pass_on(i)
    for i in near[1:-2]:
        from_mirror(i)
    pass_on(distant[0])
    from_mirror(near[-2])
    from_mirror(near[-1])
    for i in distant[1:-1]:
        pass_on(i)
    for w in weights:
        w.wait()
    for i in near[1:]:
        settle(i)
    for f in range(steps // 2):
        forward(0, f)
    pass_on(distant[-1])
    for load in late_loads:
        load.wait()
    act_from(0)
    for j in distant + near[1:]:
        og_copy(j).start()
    for i in distant[:1]:
        from_mirror(i)
    for f in range(steps // 2, steps):
        forward(0, f)
    for i in distant[1:-1]:
        from_mirror(i)
    shares_far(0)
    from_mirror(distant[-1])
    far_start(0)
    shares_own(0)
    for i in distant:
        settle(i)

    for f in range(steps):
        forward(1, f)
    for i in range(1, t):
        inner_copy(i).start()
    levels = [1 << k for k in reversed(range(n.bit_length() - 1))]

    def act_level(low):
        for j in range(low, n, 2 * low):
            act_copy(j).wait_recv()
            act_from(j)

    middle = [j for low in levels[1:-1] for j in range(low, n, 2 * low)]

    def act_next(count):
        for j in middle[:count]:
            act_copy(j).wait_recv()
            act_from(j)
        del middle[:count]
    def meanwhile():
        give_back(near[-1])
        act_next(1)

    act_level(levels[0])

    shares_far(1, meanwhile)
    far_start(1)
    far_copy(0).start()
    for i in near[1:-1]:
        give_back(i)
    shares_own(1)

    block = min(width, 512)
    chunks = width // block

    def grad_of(j, lo, hi):
        out = (gate_out, up_out, down_out)[j]
        source = j // 2

        def step(c, carry):
            at = pl.ds(pl.multiple_of(c * block, block), block)
            value = jnp.dot(
                turned_a[j], rows[source, : len(near), :, at].reshape(heights[0], block),
                preferred_element_type=F32,
            )
            value = value + jnp.dot(
                turned_b[j], rows[source, len(near) :, :, at].reshape(heights[1], block),
                preferred_element_type=F32,
            )
            out[:, at] = value.astype(BF16)
            sq = value * value
            here = squares[j]
            for k in range(block // 128):
                here = here + sq[:, k * 128 : (k + 1) * 128]
            squares[j] = here
            return carry

        lax.fori_loop(lo, hi, step, 0)

    squares[...] = jnp.zeros_like(squares)
    todo = [(j, c) for j in range(3) for c in range(chunks)]

    def spend(count):
        for j, c in todo[:count]:
            grad_of(j, c, c + 1)
        del todo[:count]

    for i in range(1, t):
        inner_copy(i).wait_recv()
    inner_tot[...] = jnp.sum(inner_tp[...], 0)
    inner_ep[0] = inner_tot[...]
    for i in range(1, n):
        inner_back(i).start()
    for k, i in enumerate(order[1]):
        spend(1)
        give_back(i)
        act_next(1)
    act_next(len(middle))
    for i in range(1, n):
        og_copy(i).wait_recv()
    og_buddy().start()
    spend(3)
    og_buddy().wait_recv()
    act_level(levels[-1])
    shared = lax.dot_general(
        act_all[...].reshape(n * toks, sh), og_all[...].reshape(n * toks, cut),
        (((0,), (0,)), ((), ())), preferred_element_type=F32,
    )
    shared_out[...] = shared
    snorm_all[0] = column_to_row(jnp.sum(shared * shared, 1, keepdims=True))
    for i in range(1, n):
        snorm_copy(i).start()
    give_back(0)
    spend(len(todo))
    for j in range(3):
        norms_out[j] = column_to_row(jnp.sum(squares[j], 1, keepdims=True))
    for i in range(1, n):
        inner_back(i).wait_recv()
    found = jnp.zeros((n, toks), F32)
    for g in range(2):
        low, size = groups[g][0] * slot, heights[g]
        block_of = lax.broadcasted_iota(jnp.int32, (n, size), 1) // slot + groups[g][0]
        row_of = lax.broadcasted_iota(jnp.int32, (n, size), 0)
        spread = jnp.zeros((n, size), F32)
        for i in groups[g]:
            spread = jnp.where(
                (block_of == i) & (row_of == i), inner_ep[i, g, :, 0:size], spread
            )
        found = found + jnp.dot(
            spread, picks[low : low + size, :].astype(F32),
            precision=lax.Precision.HIGHEST, preferred_element_type=F32,
        )
    for k in range(2):
        value = jnp.zeros((1, toks), F32)
        for i in range(n):
            value = value + jnp.where(ids_ref[k : k + 1, :] == peer(i), found[i : i + 1], 0.0)
        route_out[k : k + 1, :] = value / rw_ref[k : k + 1, :]
    for i in range(1, n):
        back_copy(i).wait_recv()
    token_out[...] = lax.dot_general(
        picks[...], back_recv[...].reshape(total, cols), (((0,), (0,)), ((), ())),
        preferred_element_type=F32,
    ).astype(BF16)
    for i in range(1, n):
        snorm_copy(i).wait_recv()
    snorm_out[...] = jnp.sum(snorm_all[...], 0)

    for i in range(1, n):
        dispatch(i).wait_send()
        to_mirror(i).wait_send()
    for i in range(1, n):
        to_buddy(i).wait_send()
        on_buddy(i).wait_send()
        og_copy(i).wait_send()
        act_copy(i).wait_send()
        inner_back(i).wait_send()
        back_copy(i).wait_send()
        snorm_copy(i).wait_send()
    for i in range(n):
        far_copy(i).wait_send()
    for i in range(1, t):
        inner_copy(i).wait_send()
    og_buddy().wait_send()
    for g in range(2):
        for k in range(2):
            pair_copy(g, k).wait_send()


def hand_over(*refs):
    count = (len(refs) - 1) // 2
    sources, targets, sem = refs[:count], refs[count : 2 * count], refs[-1]
    moves = []
    for j in sorted(range(count), key=lambda j: sources[j].size):
        moves.append(pltpu.make_async_copy(sources[j], targets[j], sem.at[j]))
        moves[-1].start()
    for move in moves:
        move.wait()


def fused(tokens, out_grad, expert_ids, route_weights, gate_proj, up_proj, down_proj, shared_act):
    n = lax.axis_size("ep")
    t = lax.axis_size("tp")
    toks, width = tokens.shape
    experts = gate_proj.shape[0] * n
    cap = 5 * toks * expert_ids.shape[1] // (4 * experts)
    slot = -(-cap // 16) * 16
    hid = gate_proj.shape[1]
    cols = width // t
    sh = shared_act.shape[1] // t
    cut = width // n
    part = toks // 2
    total = n * slot
    high, low = (n // 2 + 1) * slot, (n // 2 - 1) * slot
    vmem = pl.BlockSpec(memory_space=pltpu.VMEM)
    hbm = pl.BlockSpec(memory_space=pl.ANY)
    dma = pltpu.SemaphoreType.DMA
    results = pl.pallas_call(
        functools.partial(kernel, n, t, cap, slot),
        out_shape=(
            pltpu.VMEM((toks, cols), BF16),
            pltpu.VMEM((2, toks), F32),
            pltpu.VMEM((hid, width), BF16),
            pltpu.VMEM((hid, width), BF16),
            pltpu.VMEM((hid, width), BF16),
            pltpu.VMEM((3, 1, hid), F32),
            pltpu.VMEM((sh, cut), F32),
            pltpu.VMEM((1, sh), F32),
        ),
        in_specs=[hbm] * 8,
        out_specs=(vmem,) * 8,
        scratch_shapes=[
            pltpu.VMEM((n, 2, slot, cols), BF16),
            pltpu.VMEM((2, n, slot, width), BF16),
            pltpu.VMEM((hid, width), BF16),
            pltpu.VMEM((hid, width), BF16),
            pltpu.VMEM((hid, width), BF16),
            pltpu.VMEM((total, toks), BF16),
            pltpu.VMEM((128, toks), F32),
            pltpu.VMEM((128, toks), F32),
            pltpu.VMEM((2, high, hid), BF16),
            pltpu.VMEM((2, low, hid), BF16),
            pltpu.VMEM((3, hid, high), BF16),
            pltpu.VMEM((3, hid, low), BF16),
            pltpu.VMEM((3, hid, 128), F32),
            pltpu.VMEM((2, 2, high, cols), BF16),
            pltpu.VMEM((2, 2, high, cols), BF16),
            pltpu.VMEM((high, cols), F32),
            pltpu.VMEM((n, slot, cols), F32),
            pltpu.VMEM((n, slot, cols), BF16),
            pltpu.VMEM((n, slot, cols), BF16),
            pltpu.VMEM((n, slot, cols), BF16),
            pltpu.VMEM((n, slot, cols), BF16),
            pltpu.VMEM((t, 2, 1, high), F32),
            pltpu.VMEM((2, 1, high), F32),
            pltpu.VMEM((n, 2, 1, high), F32),
            pltpu.VMEM((2, n, part, sh), BF16),
            pltpu.VMEM((n, part, cut), BF16),
            pltpu.VMEM((2, n, part, cut), BF16),
            pltpu.VMEM((n, 1, sh), F32),
            pltpu.VMEM((2, toks), jnp.int32),
            pltpu.VMEM((2, toks), F32),
            pltpu.VMEM((toks, cols), BF16),
            pltpu.VMEM((toks, cols), BF16),
            pltpu.VMEM((toks, width), BF16),
            pltpu.VMEM((toks, width), BF16),
            dma((8 + n,)),
            dma((3,)),
            dma((n,)), dma((n,)), dma((n,)), dma((n,)), dma((2, n)), dma((2, n)),
            dma((n,)), dma((n,)), dma((n,)), dma((n,)), dma, dma,
            dma((2, 2)), dma((2, 2)), dma((n,)), dma((n,)), dma((n,)), dma((n,)),
            dma((t,)), dma((t,)), dma((n,)), dma((n,)), dma((n,)), dma((n,)),
        ],
        compiler_params=pltpu.CompilerParams(
            collective_id=0, has_side_effects=True, vmem_limit_bytes=36 * 1024 * 1024
        ),
    )(
        *[
            pltpu.with_memory_space_constraint(r, pltpu.HBM)
            for r in (
                expert_ids.T, route_weights.T, tokens, out_grad, shared_act, gate_proj, up_proj,
                down_proj,
            )
        ]
    )
    count = len(results)
    token_grad, route, gate, up, down, norms, shared, snorm = pl.pallas_call(
        hand_over,
        out_shape=[jax.ShapeDtypeStruct(r.shape, r.dtype) for r in results],
        in_specs=[vmem] * count,
        out_specs=[hbm] * count,
        scratch_shapes=[dma((count,))],
        compiler_params=pltpu.CompilerParams(vmem_limit_bytes=4 * 1024 * 1024),
    )(*[pltpu.with_memory_space_constraint(r, pltpu.VMEM) for r in results])
    return (
        token_grad, route.T, gate[None], up[None], down[None], norms.transpose(1, 0, 2), shared,
        snorm[0],
    )


def local(tokens, out_grad, expert_ids, route_weights, gate_proj, up_proj, down_proj, shared_act):
    n = lax.axis_size("ep")
    t = lax.axis_size("tp")
    toks, width = tokens.shape
    hid = gate_proj.shape[1]
    slot = -(-(5 * toks * expert_ids.shape[1] // (4 * n)) // 16) * 16
    fits = (
        gate_proj.shape[0] == 1 and expert_ids.shape[1] == 2 and t == 4 and n >= 8 and n & (n - 1) == 0 and n <= 128
        and toks % 128 == 0 and toks % 32 == 0 and width // t % 128 == 0
        and hid % 512 == 0 and n * slot % 128 == 0 and width // n % 128 == 0
        and shared_act.shape[1] // t % 128 == 0
    )
    body = fused if fits else plain
    return body(
        tokens, out_grad, expert_ids, route_weights, gate_proj, up_proj, down_proj, shared_act
    )


def solution(mesh):
    placed = (
        P("ep", None),
        P("ep", None),
        P("ep", None),
        P("ep", None),
        P("ep", "tp", None),
        P("ep", "tp", None),
        P("ep", "tp", None),
        P("ep", None),
    )
    return jax.shard_map(
        local,
        mesh=mesh,
        in_specs=placed,
        out_specs=(
            P("ep", "tp"),
            P("ep", None),
            P("ep", "tp", None),
            P("ep", "tp", None),
            P("ep", "tp", None),
            P("ep", None, "tp"),
            P("tp", "ep"),
            P("tp"),
        ),
        check_vma=False,
    )
```
